32 devices in a mesh: grp: 2 (over y), ep: 8 (over z, x), tp: 2 (over core).
Axes of the slice: x: 2, y: 2, z: 4, core: 2. Of those that a mesh axis runs over, the one named last changes fastest.
Arguments:
- tokens: bfloat16 [4096, 2048], P(('grp', 'ep', 'tp')), parts along dimension 0, may hold values from -6 to 6
- expert_ids: int32 [4096, 4], P(('grp', 'ep', 'tp')), parts along dimension 0, may hold values from 0 to 15, all different within a row; in each aligned block of 128 rows (0 to 127, 128 to 255, ...) at most 48 rows name the same one
- gate_weights: float32 [4096, 4], P(('grp', 'ep', 'tp')), parts along dimension 0, may hold values from 0.1 to 1
- norm_gain: float32 [2048], replicated, may hold values from 0.1 to 1.9
- expert_gate: bfloat16 [16, 2048, 512], P(('ep', 'tp')), may hold values from -0.125 to 0.125
- expert_up: bfloat16 [16, 2048, 512], P(('ep', 'tp')), may hold values from -0.125 to 0.125
- expert_down: bfloat16 [16, 512, 2048], P(('ep', 'tp'))
- shared_gate: bfloat16 [2048, 512], P(None, 'tp'), may hold values from -0.125 to 0.125
- shared_up: bfloat16 [2048, 512], P(None, 'tp'), may hold values from -0.125 to 0.125
- shared_down: bfloat16 [512, 2048], P('tp')
- out_gain: float32 [2048], replicated, may hold values from 0.1 to 1.9
Outputs:
- layer_out: bfloat16 [4096, 2048], P(('grp', 'ep'), 'tp'), parts along dimension 0
The draws below stay inside these ranges and needn't reach their ends.
There are 2 independent parts, one for each index of `grp`. The reference program is written for one: setup_inputs(seed, part) draws one part's arguments, and reference() takes and returns one part's arrays. A program takes and returns all parts, laid end to end along the dimension named above; an argument that names none is the same for every part. Nothing has to cross between parts.
Inputs may be any that keep to these rules, and one draw needn't show every extreme that they name: `expert_ids`: each row names 4 different experts. Among the 128 rows of one device (aligned blocks of rows), no expert is named more than 48 times, and in every draw some expert is named exactly 48 times by some device.
All inputs are finite; a program needn't handle non-finite values.
Results may differ from the reference program's by a relative error of at most 0.0085.
Values may be sent and summed in bfloat16 or wider, within the bound.
A program may use at most 64 MiB of HBM per device.

```python
import math
import jax
import jax.numpy as jnp
import numpy as np
from jax import lax

D = 2048
FF = 512
SH = 512
TOPK = 4
TOK_DEV = 128
EXPERTS = 16
CAP = 48
TOKENS = 2048
N_EP = 8
N_TP = 2


def rising_columns(key, shape, fan_in):
    base = jax.random.normal(key, shape, jnp.float32)
    columns = shape[-1]
    rise = 10.0 ** (jnp.arange(columns, dtype=jnp.float32) / (columns - 1))
    return base * rise * fan_in ** (-0.5)


def draw_expert_down(key, part):
    return rising_columns(jax.random.fold_in(key, 11), (EXPERTS, FF, D), FF).astype(jnp.bfloat16)


def draw_shared_down(key, part):
    return rising_columns(jax.random.fold_in(key, 23), (SH, D), SH).astype(jnp.bfloat16)


def block_scale(rng, shape, pieces, least, top_value):
    def one(position, shards_of):
        steps = jax.random.uniform(jax.random.fold_in(jax.random.fold_in(rng, 6), position), (shards_of,), jnp.float32, least / len(pieces), top_value / len(pieces))
        return jnp.repeat(jnp.exp(steps), shape[position] // shards_of).reshape((-1,) + (1,) * (len(shape) - position - 1))

    loudness = one(*pieces[0])
    for cut in pieces[1:]:
        loudness = loudness * one(*cut)
    return loudness


def deal_out(rng, own, number, rows, amount, top, most, skew):
    sequence = jax.random.permutation(rng, amount)
    packed, usual = shares(amount, rows * top, most, skew, True), shares(amount, rows * top, most, skew, False)
    places = jnp.arange(amount)

    def named(tallies, offset_by):
        used = int((tallies > 0).sum())
        fixed = max(1, used // 4)
        moved = fixed + (places - fixed + offset_by * (used - fixed)) % max(1, amount - fixed)
        return jnp.zeros((amount,), jnp.int32).at[sequence[jnp.where(places < fixed, places, moved)]].set(jnp.asarray(tallies, jnp.int32))

    tallies = jnp.where(number % 4 == 0, named(packed, number // 4), named(usual, number - number // 4 - 1))
    mixed = jax.random.permutation(jax.random.fold_in(own, 3), amount)
    donor, sink = mixed[0:amount // 2 * 2:2], mixed[1:amount // 2 * 2:2]
    room = jnp.minimum(tallies[donor] - 1, most - tallies[sink]) // 2
    room = jnp.where((donor == sequence[0]) | (sink == sequence[0]) | (tallies[sink] == 0), 0, jnp.maximum(room, 0))
    moved = jax.random.randint(jax.random.fold_in(own, 4), (amount // 2,), 0, 1 << 20) % (room + 1)
    tallies = tallies.at[donor].add(-moved).at[sink].add(moved)
    labels = jnp.searchsorted(jnp.cumsum(tallies), jnp.arange(rows * top), side="right").astype(jnp.int32)
    table = labels.reshape(top, rows).T
    table = table[jax.random.permutation(jax.random.fold_in(own, 1), rows)]
    offset_by = jax.random.randint(jax.random.fold_in(own, 2), (rows, 1), 0, top)
    return jnp.take_along_axis(table, (jnp.arange(top)[None, :] + offset_by) % top, axis=1)


def shares(amount, total, reach, lean, full):
    loads = [(1 << 20) // math.isqrt(standing ** lean) + 1 for standing in range(1, amount + 1)]
    largest = reach if full else min(reach, max(-(-total // amount), total * loads[0] // sum(loads)))
    least = 1 if total - largest >= amount - 1 else 0
    given, spare = [largest] + [least] * (amount - 1), total - largest - least * (amount - 1)
    while spare > 0:
        movable = [i for i in range(1, amount) if given[i] < largest] or [i for i in range(1, amount) if given[i] < reach]
        whole, remaining = sum([loads[i] for i in movable]), spare
        for i in movable:
            extra = min(reach - given[i], max(1, remaining * loads[i] // whole), spare)
            given[i] = given[i] + extra
            spare = spare - extra
    return np.array(given)


def normal_values(rng, dims, deviation, bound, pieces=(), kind=jnp.bfloat16):
    drawn = deviation * jax.random.normal(rng, dims, jnp.float32)
    if pieces:
        drawn = drawn * block_scale(rng, dims, pieces, -0.22, 0.18)
    return jnp.clip(drawn, -bound, bound).astype(kind)


def setup_inputs(seed: int = 0, part: int = 0) -> dict:
    arg_keys = jax.random.split(jax.random.key(seed), 12)
    part_keys = jax.random.split(jax.random.fold_in(arg_keys[11], part), 12)
    tokens = normal_values(part_keys[0], (TOKENS, D), 1.0, 6.0, ((0, 16),))
    expert_ids_keys = jax.random.split(jax.random.fold_in(part_keys[1], 1), TOKENS // TOK_DEV)
    expert_ids_turns = jax.random.permutation(jax.random.fold_in(part_keys[1], 3), TOKENS // TOK_DEV)
    expert_ids = jax.vmap(lambda own, number: deal_out(jax.random.fold_in(part_keys[1], 2), own, number, TOK_DEV, EXPERTS, TOPK, CAP, 2))(expert_ids_keys, expert_ids_turns).reshape((TOKENS, TOPK))
    gate_weights = jnp.clip(jnp.exp(math.log(1.0) - 2.3025851 * jax.random.uniform(part_keys[2], (TOKENS, TOPK), jnp.float32) ** block_scale(part_keys[2], (TOKENS, TOPK), ((0, 16),), -0.2, 0.2)), 0.1, 1.0)
    norm_gain = jnp.clip(1.0 + 0.18 * jax.random.normal(arg_keys[3], (D,), jnp.float32), 0.1, 1.9)
    expert_gate = normal_values(arg_keys[4], (EXPERTS, D, FF), D ** -0.5, 0.125, ((0, 16),))
    expert_up = normal_values(arg_keys[5], (EXPERTS, D, FF), D ** -0.5, 0.125, ((0, 16),))
    expert_down = draw_expert_down(jax.random.fold_in(arg_keys[11], 71), part)
    shared_gate = normal_values(arg_keys[7], (D, SH), D ** -0.5, 0.125, ((1, 2),))
    shared_up = normal_values(arg_keys[8], (D, SH), D ** -0.5, 0.125, ((1, 2),))
    shared_down = draw_shared_down(jax.random.fold_in(arg_keys[11], 71), part)
    out_gain = jnp.clip(1.0 + 0.18 * jax.random.normal(arg_keys[10], (D,), jnp.float32), 0.1, 1.9)
    return {"tokens": tokens, "expert_ids": expert_ids, "gate_weights": gate_weights, "norm_gain": norm_gain, "expert_gate": expert_gate, "expert_up": expert_up, "expert_down": expert_down, "shared_gate": shared_gate, "shared_up": shared_up, "shared_down": shared_down, "out_gain": out_gain}


def reference(tokens, expert_ids, gate_weights, norm_gain, expert_gate, expert_up, expert_down, shared_gate, shared_up, shared_down, out_gain):
    values = tokens.astype(jnp.float32)
    scale = lax.rsqrt(lax.optimization_barrier(jnp.mean(values * values, axis=1, keepdims=True)) + 1e-06)
    normed = (values * scale * norm_gain).astype(jnp.bfloat16)
    flat_ids = expert_ids.reshape(-1)
    flat_gates = gate_weights.reshape(-1)
    copy_count = TOKENS * TOPK
    most_rows = N_EP * N_TP * CAP

    def one_expert(total, inputs):
        w_gate, w_up, w_down, expert_index = inputs
        positions = jnp.nonzero(flat_ids == expert_index, size=most_rows, fill_value=copy_count)[0].astype(jnp.int32)
        valid = positions < copy_count
        clipped = jnp.minimum(positions, copy_count - 1)
        token_index = clipped // TOPK
        weight = jnp.where(valid, flat_gates[clipped], 0.0)
        rows = normed[token_index]
        gate = jnp.dot(rows, w_gate, preferred_element_type=jnp.float32)
        upper = jnp.dot(rows, w_up, preferred_element_type=jnp.float32)
        hidden = (jax.nn.silu(gate) * upper).astype(jnp.bfloat16)
        result = jnp.dot(hidden, w_down, preferred_element_type=jnp.float32).astype(jnp.bfloat16)
        total = total.at[token_index].add(result.astype(jnp.float32) * weight[:, None])
        return (total, None)
    routed, _ = lax.scan(one_expert, jnp.zeros((TOKENS, D), jnp.float32), (expert_gate, expert_up, expert_down, jnp.arange(EXPERTS, dtype=jnp.int32)))
    shared_hidden = (jax.nn.silu(jnp.dot(normed, shared_gate, preferred_element_type=jnp.float32)) * jnp.dot(normed, shared_up, preferred_element_type=jnp.float32)).astype(jnp.bfloat16)
    shared_out = jnp.dot(shared_hidden, shared_down, preferred_element_type=jnp.float32)
    mixed = (routed + shared_out).astype(jnp.bfloat16).astype(jnp.float32)
    final_scale = lax.rsqrt(lax.optimization_barrier(jnp.mean(mixed * mixed, axis=1, keepdims=True)) + 1e-06)
    return (mixed * final_scale * out_gain).astype(jnp.bfloat16)
```

```python
import functools

import jax
import jax.numpy as jnp
from jax import lax
from jax.experimental import pallas as pl
from jax.experimental.pallas import tpu as pltpu
from jax.sharding import PartitionSpec as P

MESH = pl.DeviceIdType.MESH
CHUNKS = 4
BACKS = 4
F32 = jnp.float32
BF16 = jnp.bfloat16


def ladder_kernel(
    n,
    cap,
    ids_ref,
    gates_ref,
    tok_hbm,
    gain_ref,
    out_gain_ref,
    eg_hbm,
    eu_hbm,
    ed_hbm,
    sg_hbm,
    su_hbm,
    sd_hbm,
    out_ref,
    tok,
    xo,
    xl,
    meta,
    mall,
    stage,
    xr,
    wg,
    wu,
    wd,
    sg,
    su,
    sd,
    res,
    ret,
    pt,
    acc,
    rs_send,
    rs_rx,
    home,
    home_send,
    home_rx,
    sq_send,
    sq_rx,
    tok_sem,
    load_sem,
    own_ss,
    rail_ss,
    rail_rs,
    mown_ss,
    mrail_ss,
    mrail_rs,
    md_ss,
    md_rs,
    disp_ss,
    disp_rs,
    ret_ss,
    ret_rs,
    back_ss,
    back_rs,
    ox_ss,
    ox_rs,
    h_ss,
    h_rs,
    sq_ss,
    sq_rs,
):
    levels = n // 2
    rows, width = tok.shape
    cols = width // 2
    cw, rw = width // CHUNKS, cols // BACKS
    topk = ids_ref.shape[0]
    per = 4
    experts = levels * per
    ep = lax.axis_index("ep")
    c = lax.axis_index("tp")
    oc = 1 - c
    x = ep % 2
    z = ep // 2
    ox = 1 - x
    across = z * 2 + ox
    mine = 2 * x + c
    others = (2 * x + oc, 2 * ox + c, 2 * ox + oc)
    homes = ((ep, oc), (across, c), (across, oc))
    has = (z < levels - 1, z > 0)
    beside = (jnp.minimum(ep + 2, n - 1), jnp.maximum(ep - 2, 0))
    at_end = (z == 0) | (z == levels - 1)

    def signal(e, core):
        pl.semaphore_signal(barrier, inc=1, device_id={"ep": e, "tp": core}, device_id_type=MESH)

    barrier = pltpu.get_barrier_semaphore()
    for e, core in homes:
        signal(e, core)
    for d in range(2):

        @pl.when(has[d])
        def _():
            signal(beside[d], c)

    tok_load = pltpu.make_async_copy(tok_hbm, tok, tok_sem.at[0])
    tok_load.start()

    loads = [
        (sg_hbm, sg),
        (su_hbm, su),
        (sd_hbm.at[:, pl.ds(0, cols)], sd.at[0]),
        (sd_hbm.at[:, pl.ds(cols, cols)], sd.at[1]),
        (eg_hbm.at[0], wg),
        (eu_hbm.at[0], wu),
        (ed_hbm.at[0, :, pl.ds(0, cols)], wd.at[0]),
        (ed_hbm.at[0, :, pl.ds(cols, cols)], wd.at[1]),
    ]
    loads = [pltpu.make_async_copy(s, d, load_sem.at[i]) for i, (s, d) in enumerate(loads)]
    def remote(src, dst, ssem, rsem, e, core):
        return pltpu.make_async_remote_copy(
            src_ref=src,
            dst_ref=dst,
            send_sem=ssem,
            recv_sem=rsem,
            device_id={"ep": e, "tp": core},
            device_id_type=MESH,
        )

    def dot(a, b):
        return jnp.dot(a, b, preferred_element_type=F32)

    def cs(q):
        return pl.ds(q * cw, cw)

    def ss(s):
        return pl.ds(s * rw, rw)

    expert = lax.broadcasted_iota(jnp.int32, (experts, rows), 0)
    dense = jnp.zeros((experts, rows), F32)
    member = jnp.zeros((experts, rows), F32)
    for k in range(topk):
        hit = ids_ref[k : k + 1, :] == expert
        dense += jnp.where(hit, gates_ref[k : k + 1, :], 0.0)
        member += jnp.where(hit, 1.0, 0.0)
    row = lax.broadcasted_iota(jnp.int32, (rows, rows), 0)
    lane = lax.broadcasted_iota(jnp.int32, (rows, rows), 1)
    earlier = jnp.where(row < lane, 1.0, 0.0).astype(BF16)
    eye = jnp.where(row == lane, 1.0, 0.0).astype(BF16)
    place = jnp.where(member > 0.0, dot(member.astype(BF16), earlier), -1.0)
    for k in range(levels):
        part = slice(k * per, (k + 1) * per)
        meta[z, k] = jnp.concatenate([dense[part], place[part]], axis=0)

    near = jnp.minimum(z, levels - 1 - z)
    sign = jnp.where(2 * z < levels - 1, 1, -1)
    order = []
    for i in range(levels - 1):
        paired = z + sign * (i // 2 + 1) * (1 - 2 * (i % 2))
        order.append(jnp.where(i < 2 * near, paired, z + sign * (i - near + 1)))

    def own_rail(q, d):
        return remote(
            xo.at[c, :, cs(q)],
            xl.at[z, :, cs(q)],
            own_ss.at[d],
            rail_rs.at[z, q],
            beside[d],
            c,
        )

    def own_meta(d):
        return remote(meta.at[z], meta.at[z], mown_ss.at[d], mrail_rs.at[z], beside[d], c)

    def onward(lv):
        up = lv < z
        return jnp.where(up, has[0], has[1]), jnp.where(up, beside[0], beside[1])

    def rail(lv, q):
        return remote(
            xl.at[lv, :, cs(q)],
            xl.at[lv, :, cs(q)],
            rail_ss.at[lv],
            rail_rs.at[lv, q],
            onward(lv)[1],
            c,
        )

    def rail_meta(lv):
        return remote(
            meta.at[lv], meta.at[lv], mrail_ss.at[lv], mrail_rs.at[lv], onward(lv)[1], c
        )

    def deal_meta(lv, d):
        return remote(
            meta.at[lv, z], mall.at[lv, mine], md_ss.at[lv], md_rs.at[lv], *homes[d]
        )

    def met(lv):
        three = mall.at[lv, pl.ds(0, 3)]
        return remote(three, three, md_ss.at[lv], md_rs.at[lv], ep, oc)

    def deal(lv, d, q):
        return remote(
            stage.at[lv, d, :, cs(q)],
            xr.at[lv, mine, :, cs(q)],
            disp_ss.at[lv],
            disp_rs.at[lv],
            *homes[d],
        )

    def dealt(lv):
        return remote(
            stage.at[lv], xr.at[lv, pl.ds(0, 3)], disp_ss.at[lv], disp_rs.at[lv], ep, oc
        )

    def hand(lv, d, s):
        src = (
            res.at[lv, oc, s, x],
            res.at[lv, 0, s, ox],
            res.at[lv, 1, s, ox],
        )[d]
        e, core = ((ep, oc), (across, 0), (across, 1))[d]
        return remote(
            src, ret.at[lv, mine, s], ret_ss.at[lv], ret_rs.at[lv, s], e, core
        )

    def handed(lv, s):
        three = ret.at[lv, pl.ds(0, 3), s]
        return remote(three, three, ret_ss.at[lv], ret_rs.at[lv, s], ep, oc)

    def all_handed(lv):
        three = ret.at[lv, pl.ds(0, 3)]
        return remote(three, three, ret_ss.at[lv], ret_rs.at[lv, 0], ep, oc)

    def back(lv, s, k):
        up = lv > z
        t = jnp.where(up, jnp.minimum(z + 1, levels - 1), jnp.maximum(z - 1, 0))
        slot = jnp.where(up | (lv != t), lv, levels)
        return remote(
            rs_send.at[lv, s, k],
            rs_rx.at[slot, s, k],
            back_ss.at[lv],
            back_rs.at[slot, s, k],
            t * 2 + x,
            c,
        )

    def came(slot, s, k):
        return remote(
            rs_send.at[0, s, k],
            rs_rx.at[slot, s, k],
            back_ss.at[0],
            back_rs.at[slot, s, k],
            ep,
            oc,
        )

    home_x = lambda core: remote(xo.at[core], xo.at[core], ox_ss.at[0], ox_rs.at[0], ep, oc)

    def normalise(part):
        values = tok[part, :].astype(F32)
        scale = lax.rsqrt(jnp.mean(values * values, axis=1, keepdims=True) + 1e-06)
        xo[c, part, :] = (values * scale * gain_ref[...]).astype(BF16)

    with jax.named_scope("tokload"):
        tok_load.wait()
    with jax.named_scope("norm"):
        normalise(pl.ds(0, rows))
    pl.semaphore_wait(barrier, 3 + has[0].astype(jnp.int32) + has[1].astype(jnp.int32))
    for d in range(2):

        @pl.when(has[d])
        def _():
            own_meta(d).start()
            for q in range(CHUNKS):
                own_rail(q, d).start()

    slot_f = lax.broadcasted_iota(jnp.int32, (cap, rows), 0).astype(F32)

    def selection(lv):
        picks = [
            jnp.where(meta[lv, z, pl.ds(per + j, 1), :] == slot_f, 1.0, 0.0)
            for j in (mine, *others)
        ]
        return jnp.concatenate(picks, axis=0).astype(BF16)

    def spread_meta(lv):
        mall[lv, mine] = meta[lv, z]
        for d in range(3):
            deal_meta(lv, d).start()

    def spread(lv, q, pick, block):
        got = dot(pick, block).astype(BF16)
        xr[lv, mine, :, cs(q)] = got[:cap]
        for d in range(3):
            stage[lv, d, :, cs(q)] = got[(d + 1) * cap : (d + 2) * cap]
        for d in (1, 2, 0):
            deal(lv, d, q).start()

    spread_meta(z)
    pick = selection(z)
    for q in range(CHUNKS):
        spread(z, q, pick, xo[c, :, cs(q)])
    home_x(c).start()
    for load in loads:
        load.start()

    def silu_mul(g, u):
        return (g / (1.0 + jnp.exp(-g)) * u).astype(BF16)

    def compute(lv):
        met(lv).wait_recv()
        weight = jnp.concatenate(
            [
                jnp.sum(
                    jnp.where(
                        mall[lv, j, pl.ds(per + mine, 1), :] == slot_f,
                        mall[lv, j, pl.ds(mine, 1), :],
                        0.0,
                    ),
                    axis=1,
                    keepdims=True,
                )
                for j in range(per)
            ],
            axis=0,
        )
        spot = lax.broadcasted_iota(jnp.int32, (rows, per * cap), 1)
        for k in range(2):
            column = lax.dot_general(
                eye,
                mall[lv, 2 * x + k].astype(BF16),
                (((1,), (1,)), ((), ())),
                preferred_element_type=F32,
            ).astype(jnp.int32)
            want = column[:, per : per + 1]
            for j in range(1, per):
                want = jnp.where(spot >= cap * j, column[:, per + j : per + j + 1] + cap * j, want)
            pt[lv, k] = jnp.where(want == spot, 1.0, 0.0).astype(BF16)
        with jax.named_scope("wait_dealt"):
            dealt(lv).wait_recv()
        xs = xr[lv].reshape(per * cap, width)
        hidden = silu_mul(dot(xs, wg[...]), dot(xs, wu[...]))
        for s in range(BACKS):
            for h in range(2):
                out = (dot(hidden, wd[h, :, ss(s)]) * weight).astype(BF16)
                res[lv, h, s] = out.reshape(2, 2 * cap, rw)
            ret[lv, mine, s] = res[lv, c, s, x]

    def send_back(lv, s):
        for d in (1, 2, 0):
            hand(lv, d, s).start()

    def merge(lv, s, k):
        got = jnp.concatenate(
            [ret[lv, j, s, k * cap : (k + 1) * cap, :] for j in range(per)], axis=0
        )
        acc[k] = dot(pt[lv, k], got)

    def add(slot, s, k):
        with jax.named_scope(f"wait_came#s={s}"):
            came(slot, s, k).wait_recv()
        acc[k] += rs_rx[slot, s, k].astype(F32)

    def ready(lv, s):
        with jax.named_scope(f"wait_handed#s={s}"):
            handed(lv, s).wait_recv()

    def give(lv, s):
        ready(lv, s)
        for k in range(2):
            merge(lv, s, k)

            @pl.when(jnp.where(lv > z, has[1], has[0]))
            def _():
                add(lv, s, k)

            rs_send[lv, s, k] = acc[k].astype(BF16)
            back(lv, s, k).start()

    def meet(lv):
        rail_meta(lv).wait_recv()

        @pl.when(onward(lv)[0])
        def _():
            rail_meta(lv).start()

        spread_meta(lv)
        return selection(lv)

    def step(lv, q, pick):
        with jax.named_scope(f"wait_rail#q={q}"):
            rail(lv, q).wait_recv()

        @pl.when(onward(lv)[0])
        def _():
            rail(lv, q).start()

        spread(lv, q, pick, xl[lv, :, cs(q)])

    home_copy = remote(home_send, home_rx, h_ss.at[0], h_rs.at[0], ep, oc)

    def share():
        home_x(oc).wait_recv()
        xs = xo[...].reshape(2 * rows, width)
        shared = silu_mul(dot(xs, sg[...]), dot(xs, su[...]))
        home_send[...] = dot(shared, sd[oc])
        home[...] = dot(shared, sd[c])
        home_copy.start()

    def sent_rails():
        home_x(c).wait_send()
        for d in range(2):

            @pl.when(has[d])
            def _():
                own_meta(d).wait_send()
                remote(xo.at[c], xl.at[z], own_ss.at[d], rail_rs.at[z, 0], ep, oc).wait_send()

        for lv in order:

            @pl.when(onward(lv)[0])
            def _():
                rail_meta(lv).wait_send()
                remote(xl.at[lv], xl.at[lv], rail_ss.at[lv], rail_rs.at[lv, 0], ep, oc).wait_send()

    def sent_deals(lv):
        met(lv).wait_send()
        dealt(lv).wait_send()

    def sent_back(lv):
        all_handed(lv).wait_send()

    near0, near1, near2 = order
    def loaded():
        for load in loads:
            load.wait()

    @pl.when(at_end)
    def _():
        with jax.named_scope("gather0"):
            pick = meet(near0)
            for q in range(CHUNKS):
                step(near0, q, pick)
        pick = meet(near1)
        step(near1, 0, pick)
        step(near1, 1, pick)
        loaded()
        with jax.named_scope("compute0"):
            compute(near0)
        send_back(near0, 0)
        step(near1, 2, pick)
        send_back(near0, 1)
        step(near1, 3, pick)
        send_back(near0, 2)
        pick = meet(near2)
        with jax.named_scope("give0"):
            give(near0, 0)
        with jax.named_scope("share"):
            share()
        step(near2, 0, pick)
        with jax.named_scope("computez"):
            compute(z)
        step(near2, 1, pick)
        with jax.named_scope("give0"):
            give(near0, 1)
        step(near2, 2, pick)
        with jax.named_scope("compute1"):
            compute(near1)
        with jax.named_scope("give0"):
            give(near0, 2)
        step(near2, 3, pick)
        send_back(near1, 0)
        send_back(near1, 1)
        with jax.named_scope("compute2"):
            compute(near2)
        for s in range(BACKS):
            send_back(near2, s)
        send_back(near1, 2)
        send_back(near1, 3)
        send_back(near0, 3)
        for s in range(BACKS):
            send_back(z, s)
        for lv, s in (
            (near1, 0),
            (near1, 1),
            (near2, 0),
            (near2, 1),
            (near2, 2),
            (near2, 3),
            (near1, 2),
            (near1, 3),
            (near0, 3),
        ):
            with jax.named_scope(f"give{0 if lv is near0 else 1 if lv is near1 else 2}#s={s}"):
                give(lv, s)
            if lv is near1 and s == 0:
                with jax.named_scope("sent"):
                    sent_rails()
                    for v in (z, near0, near1):
                        sent_deals(v)
        for lv in order:
            sent_back(lv)
        sent_deals(near2)

    @pl.when(jnp.logical_not(at_end))
    def _():
        for lv in order:
            with jax.named_scope("gather"):
                pick = meet(lv)
                for q in range(CHUNKS):
                    step(lv, q, pick)
        loaded()
        for k, lv in enumerate((near0, near1)):
            with jax.named_scope(f"compute{k}"):
                compute(lv)
            if k == 0:
                for s in range(BACKS):
                    send_back(lv, s)
        with jax.named_scope("share"):
            share()
        with jax.named_scope("computez"):
            compute(z)
        with jax.named_scope("compute2"):
            compute(near2)
        for lv in (near2, near1, z):
            for s in range(BACKS):
                send_back(lv, s)
        with jax.named_scope("sent"):
            sent_rails()
            for lv in (z, *order):
                sent_deals(lv)
            sent_back(near0)
        for lv, s in (
            (near0, 0),
            (near0, 1),
            (near2, 0),
            (near2, 1),
            (near1, 0),
            (near2, 2),
            (near1, 1),
            (near2, 3),
            (near1, 2),
            (near0, 2),
            (near1, 3),
            (near0, 3),
        ):
            with jax.named_scope(f"give{0 if lv is near0 else 1 if lv is near1 else 2}#s={s}"):
                give(lv, s)
        for lv in (near1, near2):
            sent_back(lv)

    home_copy.wait_recv()
    home[...] += home_rx[...]
    square = [jnp.zeros((rows, 1), F32) for _ in range(2)]
    for s in range(BACKS):
        ready(z, s)
        for k in range(2):
            merge(z, s, k)
            for d, slot in ((1, z), (0, levels)):

                @pl.when(has[d])
                def _():
                    add(slot, s, k)

            part = pl.ds(k * rows, rows)
            total = (home[part, ss(s)] + acc[k]).astype(BF16).astype(F32)
            home[part, ss(s)] = total
            square[k] += jnp.sum(total * total, axis=1, keepdims=True)
    for k in range(2):
        sq_send[k * rows : (k + 1) * rows, :] = jnp.broadcast_to(square[k], (rows, 128))
    squares = remote(sq_send, sq_rx, sq_ss.at[0], sq_rs.at[0], ep, oc)
    squares.start()
    with jax.named_scope("wait_sq"):
        squares.wait_recv()
    with jax.named_scope("final"):
      final = lax.rsqrt((sq_send[...] + sq_rx[...])[:, :1] / width + 1e-06)
      out_ref[...] = (home[...] * final * out_gain_ref[c]).astype(BF16)

    with jax.named_scope("sentend"):
        for lv in order:
            remote(rs_send.at[lv], rs_rx.at[lv], back_ss.at[lv], back_rs.at[lv, 0, 0], ep, oc).wait_send()
        sent_back(z)
        home_copy.wait_send()
        squares.wait_send()


def ladder_local(
    n,
    cap,
    tokens,
    expert_ids,
    gate_weights,
    norm_gain,
    expert_gate,
    expert_up,
    expert_down,
    shared_gate,
    shared_up,
    shared_down,
    out_gain,
):
    rows, width = tokens.shape
    ff = expert_gate.shape[2]
    sh = shared_gate.shape[1]
    cols = width // 2
    levels = n // 2
    rw = cols // BACKS
    dma = pltpu.SemaphoreType.DMA
    vmem = pl.BlockSpec(memory_space=pltpu.VMEM)
    hbm = pl.BlockSpec(memory_space=pl.ANY)
    return pl.pallas_call(
        functools.partial(ladder_kernel, n, cap),
        out_shape=pltpu.VMEM((2 * rows, cols), BF16),
        in_specs=[vmem] * 2 + [hbm] + [vmem] * 2 + [hbm] * 6,
        out_specs=vmem,
        scratch_shapes=[
            pltpu.VMEM((rows, width), BF16),
            pltpu.VMEM((2, rows, width), BF16),
            pltpu.VMEM((levels, rows, width), BF16),
            pltpu.VMEM((levels, levels, 8, rows), F32),
            pltpu.VMEM((levels, 4, 8, rows), F32),
            pltpu.VMEM((levels, 3, cap, width), BF16),
            pltpu.VMEM((levels, 4, cap, width), BF16),
            pltpu.VMEM((width, ff), BF16),
            pltpu.VMEM((width, ff), BF16),
            pltpu.VMEM((2, ff, cols), BF16),
            pltpu.VMEM((width, sh), BF16),
            pltpu.VMEM((width, sh), BF16),
            pltpu.VMEM((2, sh, cols), BF16),
            pltpu.VMEM((levels, 2, BACKS, 2, 2 * cap, rw), BF16),
            pltpu.VMEM((levels, 4, BACKS, 2 * cap, rw), BF16),
            pltpu.VMEM((levels, 2, rows, 4 * cap), BF16),
            pltpu.VMEM((2, rows, rw), F32),
            pltpu.VMEM((levels, BACKS, 2, rows, rw), BF16),
            pltpu.VMEM((levels + 1, BACKS, 2, rows, rw), BF16),
            pltpu.VMEM((2 * rows, cols), F32),
            pltpu.VMEM((2 * rows, cols), F32),
            pltpu.VMEM((2 * rows, cols), F32),
            pltpu.VMEM((2 * rows, 128), F32),
            pltpu.VMEM((2 * rows, 128), F32),
            dma((1,)),
            dma((8,)),
            dma((2,)),
            dma((levels,)),
            dma((levels, CHUNKS)),
            dma((2,)),
            dma((levels,)),
            dma((levels,)),
            dma((levels,)),
            dma((levels,)),
            dma((levels,)),
            dma((levels,)),
            dma((levels,)),
            dma((levels, BACKS)),
            dma((levels,)),
            dma((levels + 1, BACKS, 2)),
            dma((1,)),
            dma((1,)),
            dma((1,)),
            dma((1,)),
            dma((1,)),
            dma((1,)),
        ],
        compiler_params=pltpu.CompilerParams(
            collective_id=0, has_side_effects=True, vmem_limit_bytes=60 * 1024 * 1024
        ),
    )(
        expert_ids.T,
        gate_weights.T,
        tokens,
        norm_gain.reshape(1, width),
        out_gain.reshape(2, 1, cols),
        expert_gate,
        expert_up,
        expert_down,
        shared_gate,
        shared_up,
        shared_down,
    )


TOPK = 4


def expert_work(received, expert_gate, expert_up, expert_down):
    gate = jnp.einsum("slcd,ldf->slcf", received, expert_gate, preferred_element_type=jnp.float32)
    upper = jnp.einsum("slcd,ldf->slcf", received, expert_up, preferred_element_type=jnp.float32)
    hidden = (jax.nn.silu(gate) * upper).astype(jnp.bfloat16)
    return jnp.einsum(
        "slcf,lfd->slcd", hidden, expert_down, preferred_element_type=jnp.float32
    ).astype(jnp.bfloat16)


def local(
    tokens,
    expert_ids,
    gate_weights,
    norm_gain,
    expert_gate,
    expert_up,
    expert_down,
    shared_gate,
    shared_up,
    shared_down,
    out_gain,
):
    local_rows = tokens.shape[0]
    width = tokens.shape[1]
    ep_count = lax.axis_size("ep")
    tp_count = lax.axis_size("tp")
    device_count = ep_count * tp_count
    local_experts = expert_gate.shape[0]
    expert_count = device_count * local_experts
    capacity = 3 * local_rows * TOPK // (2 * expert_count)
    values = tokens.astype(jnp.float32)
    scale = lax.rsqrt(jnp.mean(values * values, axis=1, keepdims=True) + 1e-06)
    normed = (values * scale * norm_gain).astype(jnp.bfloat16)
    flat_ids = expert_ids.reshape(-1)
    one_hot = (flat_ids[:, None] == jnp.arange(expert_count, dtype=jnp.int32)[None, :]).astype(
        jnp.int32
    )
    earlier = jnp.cumsum(one_hot, axis=0) - one_hot
    slot_index = jnp.sum(earlier * one_hot, axis=1)
    target = flat_ids * capacity + slot_index
    copy_rows = normed[jnp.arange(local_rows * TOPK, dtype=jnp.int32) // TOPK]
    outgoing = jnp.zeros((expert_count * capacity, width), jnp.bfloat16).at[target].set(copy_rows)
    sending = outgoing.reshape(device_count, local_experts * capacity, width)
    received = lax.all_to_all(sending, ("ep", "tp"), split_axis=0, concat_axis=0, tiled=True)
    received = received.reshape(device_count, local_experts, capacity, width)
    results = expert_work(received, expert_gate, expert_up, expert_down)
    results = results.reshape(device_count, local_experts * capacity, width)
    returned = lax.all_to_all(results, ("ep", "tp"), split_axis=0, concat_axis=0, tiled=True)
    returned = returned.reshape(expert_count * capacity, width)
    picked = returned[target].astype(jnp.float32).reshape(local_rows, TOPK, width)
    routed = jnp.sum(picked * gate_weights[:, :, None], axis=1)
    piece = lax.all_gather(normed, "tp", axis=0, tiled=True)
    gate = jnp.dot(piece, shared_gate, preferred_element_type=jnp.float32)
    upper = jnp.dot(piece, shared_up, preferred_element_type=jnp.float32)
    shared_hidden = (jax.nn.silu(gate) * upper).astype(jnp.bfloat16)
    shared_out = lax.psum_scatter(
        jnp.dot(shared_hidden, shared_down, preferred_element_type=jnp.float32),
        "tp",
        scatter_dimension=0,
        tiled=True,
    )
    mixed = (routed + shared_out).astype(jnp.bfloat16)
    mixed_values = mixed.astype(jnp.float32)
    final_scale = lax.rsqrt(jnp.mean(mixed_values * mixed_values, axis=1, keepdims=True) + 1e-06)
    normalized = (mixed_values * final_scale * out_gain).astype(jnp.bfloat16)
    return lax.all_to_all(normalized, "tp", split_axis=1, concat_axis=0, tiled=True)


def solution(mesh):
    in_specs = (
        P(("grp", "ep", "tp"), None),
        P(("grp", "ep", "tp"), None),
        P(("grp", "ep", "tp"), None),
        P(),
        P(("ep", "tp"), None, None),
        P(("ep", "tp"), None, None),
        P(("ep", "tp"), None, None),
        P(None, "tp"),
        P(None, "tp"),
        P("tp", None),
        P(),
    )
    out_specs = P(("grp", "ep"), "tp")
    n, tp = mesh.shape["ep"], mesh.shape["tp"]

    def run(*args):
        tokens, expert_gate = args[0], args[4]
        rows = tokens.shape[0] // mesh.size
        experts = expert_gate.shape[0]
        cap = 3 * rows * args[1].shape[1] // (2 * experts)
        dense = experts == n * tp and experts <= 8 * args[1].shape[1]
        dense = dense and tp == 2 and n == 8 and rows == 128 and cap % 16 == 0
        body = functools.partial(ladder_local, n, cap) if dense else local
        return jax.shard_map(
            body, mesh=mesh, in_specs=in_specs, out_specs=out_specs, check_vma=False
        )(*args)

    return run
```

```python
import functools

import jax
import jax.numpy as jnp
from jax import lax
from jax.experimental import pallas as pl
from jax.experimental.pallas import tpu as pltpu
from jax.sharding import PartitionSpec as P

MESH = pl.DeviceIdType.MESH
CHUNKS = 4
BACKS = 4


def pieces(s, k, rows):
    if s < BACKS - 1:
        return [(2 * s + k, 0, rows)]
    half = rows // 2
    return [(2 * s + 2 * k + i, i * half, half) for i in range(2)]
F32 = jnp.float32
BF16 = jnp.bfloat16


def ladder_kernel(
    n,
    cap,
    ids_hbm,
    gates_hbm,
    tok_hbm,
    gain_hbm,
    out_gain_hbm,
    eg_hbm,
    eu_hbm,
    ed_hbm,
    sg_hbm,
    su_hbm,
    sd_hbm,
    out_ref,
    ids_ref,
    gates_ref,
    gain_ref,
    out_gain_ref,
    tok,
    xo,
    xl,
    meta,
    mall,
    stage,
    xr,
    wg,
    wu,
    wd,
    sg,
    su,
    sd,
    res,
    ret,
    pt,
    pc,
    comb,
    mallp,
    rh,
    ro,
    cross_tx,
    cross_rx,
    acc,
    rs_send,
    rs_rx,
    home,
    home_send,
    home_rx,
    sq_send,
    sq_rx,
    tok_sem,
    load_sem,
    own_ss,
    rail_ss,
    rail_rs,
    mown_ss,
    mrail_ss,
    mrail_rs,
    md_ss,
    md_rs,
    disp_ss,
    disp_rs,
    ret_ss,
    ret_rs,
    back_ss,
    back_rs,
    mp_ss,
    mp_rs,
    rh_ss,
    rh_rs,
    ro_ss,
    ro_rs,
    cross_ss,
    cross_rs,
    ox_ss,
    ox_rs,
    h_ss,
    h_rs,
    sq_ss,
    sq_rs,
):
    levels = n // 2
    rows, width = tok.shape
    cols = width // 2
    cw, rw = width // CHUNKS, cols // BACKS
    topk = ids_ref.shape[0]
    per = 4
    experts = levels * per
    ep = lax.axis_index("ep")
    c = lax.axis_index("tp")
    oc = 1 - c
    x = ep % 2
    z = ep // 2
    ox = 1 - x
    across = z * 2 + ox
    mine = 2 * x + c
    others = (2 * x + oc, 2 * ox + c, 2 * ox + oc)
    homes = ((ep, oc), (across, c), (across, oc))
    has = (z < levels - 1, z > 0)
    beside = (jnp.minimum(ep + 2, n - 1), jnp.maximum(ep - 2, 0))
    at_end = (z == 0) | (z == levels - 1)

    firsts = [(ids_hbm, ids_ref), (gates_hbm, gates_ref), (tok_hbm, tok), (gain_hbm, gain_ref)]
    firsts.append((out_gain_hbm, out_gain_ref))
    firsts = [pltpu.make_async_copy(a, b, tok_sem.at[i]) for i, (a, b) in enumerate(firsts)]
    for load in firsts:
        load.start()

    def signal(e, core):
        pl.semaphore_signal(barrier, inc=1, device_id={"ep": e, "tp": core}, device_id_type=MESH)

    barrier = pltpu.get_barrier_semaphore()
    for e, core in homes:
        signal(e, core)
    for d in range(2):

        @pl.when(has[d])
        def _():
            signal(beside[d], c)

    loads = [
        (sg_hbm, sg),
        (su_hbm, su),
        (sd_hbm.at[:, pl.ds(0, cols)], sd.at[0]),
        (sd_hbm.at[:, pl.ds(cols, cols)], sd.at[1]),
        (eg_hbm.at[0], wg),
        (eu_hbm.at[0], wu),
        (ed_hbm.at[0, :, pl.ds(0, cols)], wd.at[0]),
        (ed_hbm.at[0, :, pl.ds(cols, cols)], wd.at[1]),
    ]
    loads = [pltpu.make_async_copy(s, d, load_sem.at[i]) for i, (s, d) in enumerate(loads)]
    def remote(src, dst, ssem, rsem, e, core):
        return pltpu.make_async_remote_copy(
            src_ref=src,
            dst_ref=dst,
            send_sem=ssem,
            recv_sem=rsem,
            device_id={"ep": e, "tp": core},
            device_id_type=MESH,
        )

    def dot(a, b):
        return jnp.dot(a, b, preferred_element_type=F32)

    def cs(q):
        return pl.ds(q * cw, cw)

    def ss(s):
        return pl.ds(s * rw, rw)

    for load in firsts[:2]:
        load.wait()
    expert = lax.broadcasted_iota(jnp.int32, (experts, rows), 0)
    dense = jnp.zeros((experts, rows), F32)
    member = jnp.zeros((experts, rows), F32)
    for k in range(topk):
        hit = ids_ref[k : k + 1, :] == expert
        dense += jnp.where(hit, gates_ref[k : k + 1, :], 0.0)
        member += jnp.where(hit, 1.0, 0.0)
    row = lax.broadcasted_iota(jnp.int32, (rows, rows), 0)
    lane = lax.broadcasted_iota(jnp.int32, (rows, rows), 1)
    earlier = jnp.where(row < lane, 1.0, 0.0).astype(BF16)
    eye = jnp.where(row == lane, 1.0, 0.0).astype(BF16)
    place = jnp.where(member > 0.0, dot(member.astype(BF16), earlier), -1.0)
    for k in range(levels):
        part = slice(k * per, (k + 1) * per)
        meta[z, k] = jnp.concatenate([dense[part], place[part]], axis=0)

    near = jnp.minimum(z, levels - 1 - z)
    sign = jnp.where(2 * z < levels - 1, 1, -1)
    order = []
    for i in range(levels - 1):
        paired = z + sign * (i // 2 + 1) * (1 - 2 * (i % 2))
        order.append(jnp.where(i < 2 * near, paired, z + sign * (i - near + 1)))

    pair = z + 1 - 2 * (z % 2)
    inner = jnp.where(2 * z < levels - 1, levels, z)

    def own_rail(q, d):
        return remote(
            xo.at[c, :, cs(q)],
            xl.at[z, :, cs(q)],
            own_ss.at[d],
            rail_rs.at[z, q],
            beside[d],
            c,
        )

    def own_meta(d):
        return remote(meta.at[z], meta.at[z], mown_ss.at[d], mrail_rs.at[z], beside[d], c)

    def onward(lv):
        up = lv < z
        return jnp.where(up, has[0], has[1]), jnp.where(up, beside[0], beside[1])

    def rail(lv, q):
        return remote(
            xl.at[lv, :, cs(q)],
            xl.at[lv, :, cs(q)],
            rail_ss.at[lv],
            rail_rs.at[lv, q],
            onward(lv)[1],
            c,
        )

    def rail_meta(lv):
        return remote(
            meta.at[lv], meta.at[lv], mrail_ss.at[lv], mrail_rs.at[lv], onward(lv)[1], c
        )

    def deal_meta(lv, d):
        return remote(
            meta.at[lv, z], mall.at[lv, mine], md_ss.at[lv], md_rs.at[lv], *homes[d]
        )

    def met(lv):
        three = mall.at[lv, pl.ds(0, 3)]
        return remote(three, three, md_ss.at[lv], md_rs.at[lv], ep, oc)

    def deal(lv, d, q):
        return remote(
            stage.at[lv, d, :, cs(q)],
            xr.at[lv, mine, :, cs(q)],
            disp_ss.at[lv],
            disp_rs.at[lv],
            *homes[d],
        )

    def dealt(lv):
        return remote(
            stage.at[lv], xr.at[lv, pl.ds(0, 3)], disp_ss.at[lv], disp_rs.at[lv], ep, oc
        )

    def hand(lv, d, s):
        src = (
            res.at[lv, oc, s, x],
            res.at[lv, 0, s, ox],
            res.at[lv, 1, s, ox],
        )[d]
        e, core = ((ep, oc), (across, 0), (across, 1))[d]
        return remote(
            src, ret.at[lv, mine, s], ret_ss.at[lv], ret_rs.at[lv, s], e, core
        )

    def handed(lv, s):
        three = ret.at[lv, pl.ds(0, 3), s]
        return remote(three, three, ret_ss.at[lv], ret_rs.at[lv, s], ep, oc)

    def all_handed(lv):
        three = ret.at[lv, pl.ds(0, 3)]
        return remote(three, three, ret_ss.at[lv], ret_rs.at[lv, 0], ep, oc)

    def back(lv, s, k, piece):
        up = lv > z
        t = jnp.where(up, jnp.minimum(z + 1, levels - 1), jnp.maximum(z - 1, 0))
        slot = jnp.where(up | (lv != t), lv, levels)
        i, first, count = piece
        return remote(
            rs_send.at[lv, s, k, pl.ds(first, count)],
            rs_rx.at[slot, s, k, pl.ds(first, count)],
            back_ss.at[lv],
            back_rs.at[slot, i],
            t * 2 + x,
            c,
        )

    def deal_pair(d):
        return remote(
            meta.at[z, pair], mallp.at[mine], mp_ss.at[0], mp_rs.at[0], *homes[d]
        )

    def pair_met():
        three = mallp.at[pl.ds(0, 3)]
        return remote(three, three, mp_ss.at[0], mp_rs.at[0], ep, oc)

    def hand_pair(lv, s, h, whole):
        src, dst = res.at[lv, h, s], rh.at[c, s]
        if not whole:
            src, dst = src.at[ox], dst.at[ox]
        return remote(src, dst, rh_ss.at[0], rh_rs.at[s], pair * 2 + x, h)

    def paired(s, whole):
        both = rh.at[pl.ds(0, 2), s] if whole else rh.at[pl.ds(0, 2), s, 0]
        return remote(both, both, rh_ss.at[0], rh_rs.at[s], ep, oc)

    def hand_own(s):
        return remote(res.at[z, oc, s], ro.at[c, s], ro_ss.at[0], ro_rs.at[s], ep, oc)

    def cross_copy(s, k):
        return remote(
            cross_tx.at[s, k],
            cross_rx.at[s, k],
            cross_ss.at[0],
            cross_rs.at[s, k],
            across,
            c,
        )

    def came(slot, s, k, piece):
        i, first, count = piece
        part = rs_rx.at[slot, s, k, pl.ds(first, count)]
        return remote(part, part, back_ss.at[0], back_rs.at[slot, i], ep, oc)

    home_x = lambda core: remote(xo.at[core], xo.at[core], ox_ss.at[0], ox_rs.at[0], ep, oc)

    def normalise(part):
        values = tok[part, :].astype(F32)
        scale = lax.rsqrt(jnp.mean(values * values, axis=1, keepdims=True) + 1e-06)
        xo[c, part, :] = (values * scale * gain_ref[...]).astype(BF16)

    with jax.named_scope("tokload"):
        for load in firsts[2:]:
            load.wait()
    with jax.named_scope("norm"):
        normalise(pl.ds(0, rows))
    pl.semaphore_wait(barrier, 3 + has[0].astype(jnp.int32) + has[1].astype(jnp.int32))
    for d in range(2):

        @pl.when(has[d])
        def _():
            own_meta(d).start()
            for q in range(CHUNKS):
                own_rail(q, d).start()

    slot_f = lax.broadcasted_iota(jnp.int32, (cap, rows), 0).astype(F32)

    def selection(lv):
        picks = [
            jnp.where(meta[lv, z, pl.ds(per + j, 1), :] == slot_f, 1.0, 0.0)
            for j in (mine, *others)
        ]
        return jnp.concatenate(picks, axis=0).astype(BF16)

    def spread_meta(lv):
        mall[lv, mine] = meta[lv, z]
        for d in range(3):
            deal_meta(lv, d).start()

    def spread(lv, q, pick, block):
        got = dot(pick, block).astype(BF16)
        xr[lv, mine, :, cs(q)] = got[:cap]
        for d in range(3):
            stage[lv, d, :, cs(q)] = got[(d + 1) * cap : (d + 2) * cap]
        for d in (1, 2, 0):
            deal(lv, d, q).start()

    spread_meta(z)
    mallp[mine] = meta[z, pair]
    for d in range(3):
        deal_pair(d).start()
    pick = selection(z)
    for q in range(CHUNKS):
        spread(z, q, pick, xo[c, :, cs(q)])
    home_x(c).start()
    for load in loads:
        load.start()

    def silu_mul(g, u):
        return (g / (1.0 + jnp.exp(-g)) * u).astype(BF16)

    def columns(m):
        return lax.dot_general(
            eye, m.astype(BF16), (((1,), (1,)), ((), ())), preferred_element_type=F32
        ).astype(jnp.int32)

    def two(m):
        col = columns(m)
        return [
            jnp.where(x == 0, col[:, per + j : per + j + 1], col[:, per + 2 + j : per + 3 + j])
            for j in range(2)
        ]

    def expander(wants):
        spot = lax.broadcasted_iota(jnp.int32, (rows, len(wants) * cap), 1)
        want = wants[0]
        for j in range(1, len(wants)):
            want = jnp.where(spot >= cap * j, wants[j] + cap * j, want)
        return jnp.where(want == spot, 1.0, 0.0).astype(BF16)

    def compute(lv, kind):
        met(lv).wait_recv()
        weight = jnp.concatenate(
            [
                jnp.sum(
                    jnp.where(
                        mall[lv, j, pl.ds(per + mine, 1), :] == slot_f,
                        mall[lv, j, pl.ds(mine, 1), :],
                        0.0,
                    ),
                    axis=1,
                    keepdims=True,
                )
                for j in range(per)
            ],
            axis=0,
        )
        for k in range(2):
            if kind == "far":
                col = columns(mall[lv, 2 * x + k])
                pt[lv, k] = expander([col[:, per + j : per + j + 1] for j in range(per)])
            elif kind == "chain":
                pc[k] = expander(two(mall[lv, 2 * x + k]))
        if kind == "own":
            pair_met().wait_recv()
            for r, rail_x in enumerate((x, ox)):
                for k in range(2):
                    j = 2 * rail_x + k
                    comb[r, k] = expander(two(mall[lv, j]) + two(mallp[j]))
        with jax.named_scope("wait_dealt"):
            dealt(lv).wait_recv()
        xs = xr[lv].reshape(per * cap, width)
        hidden = silu_mul(dot(xs, wg[...]), dot(xs, wu[...]))
        for s in range(BACKS):
            for h in range(2):
                out = (dot(hidden, wd[h, :, ss(s)]) * weight).astype(BF16)
                res[lv, h, s] = out.reshape(2, 2 * cap, rw)
            if kind in ("far", "chain"):
                ret[lv, mine, s] = res[lv, c, s, x]
            elif kind == "own":
                ro[c, s] = res[lv, c, s]

    def send_back(lv, s):
        for d in (1, 2, 0):
            hand(lv, d, s).start()

    def merge(lv, s, k):
        got = jnp.concatenate(
            [ret[lv, j, s, k * cap : (k + 1) * cap, :] for j in range(per)], axis=0
        )
        acc[k] = dot(pt[lv, k], got)

    def add(slot, s, k, piece):
        with jax.named_scope(f"wait_came#s={s}"):
            came(slot, s, k, piece).wait_recv()
        part = pl.ds(piece[1], piece[2])
        acc[k, part, :] += rs_rx[slot, s, k, part, :].astype(F32)

    def ready(lv, s):
        with jax.named_scope(f"wait_handed#s={s}"):
            handed(lv, s).wait_recv()

    def pass_on(lv, s, k, piece):
        part = pl.ds(piece[1], piece[2])
        rs_send[lv, s, k, part, :] = acc[k, part, :].astype(BF16)
        back(lv, s, k, piece).start()

    def give(lv, s):
        ready(lv, s)
        for k in range(2):
            merge(lv, s, k)
            for piece in pieces(s, k, rows):

                @pl.when(jnp.where(lv > z, has[1], has[0]))
                def _():
                    add(lv, s, k, piece)

                pass_on(lv, s, k, piece)

    def part_of(ref, j, s, r, k):
        return ref[j, s, r, k * cap : (k + 1) * cap, :]

    def give_chain(lv, s):
        one = ret.at[lv, 0, s]
        remote(one, one, ret_ss.at[lv], ret_rs.at[lv, s], ep, oc).wait_recv()
        for k in range(2):
            got = jnp.concatenate(
                [ret[lv, 2 * x + j, s, k * cap : (k + 1) * cap, :] for j in range(2)], axis=0
            )
            acc[k] = dot(pc[k], got)
            for piece in pieces(s, k, rows):
                add(lv, s, k, piece)
                pass_on(lv, s, k, piece)

    def cross(s, whole):
        hand = remote(ro.at[0, s], ro.at[0, s], ro_ss.at[0], ro_rs.at[s], ep, oc)
        hand.wait_recv()
        with jax.named_scope("wait_paired"):
            paired(s, whole).wait_recv()
        for k in range(2):
            got = jnp.concatenate(
                [part_of(ref, j, s, ox, k) for ref in (ro, rh) for j in range(2)], axis=0
            )
            cross_tx[s, k] = dot(comb[1, k], got).astype(BF16)
            cross_copy(s, k).start()

    def settle(s, k, whole):
        refs = (ro, rh) if whole else (ro,)
        got = jnp.concatenate([part_of(ref, j, s, x, k) for ref in refs for j in range(2)], axis=0)
        acc[k] = dot(comb[0, k, :, : got.shape[0]], got)

    def meet(lv):
        rail_meta(lv).wait_recv()

        @pl.when(onward(lv)[0])
        def _():
            rail_meta(lv).start()

        spread_meta(lv)
        return selection(lv)

    def step(lv, q, pick):
        with jax.named_scope(f"wait_rail#q={q}"):
            rail(lv, q).wait_recv()

        @pl.when(onward(lv)[0])
        def _():
            rail(lv, q).start()

        spread(lv, q, pick, xl[lv, :, cs(q)])

    home_copy = remote(home_send, home_rx, h_ss.at[0], h_rs.at[0], ep, oc)

    def share():
        home_x(oc).wait_recv()
        xs = xo[...].reshape(2 * rows, width)
        shared = silu_mul(dot(xs, sg[...]), dot(xs, su[...]))
        home_send[...] = dot(shared, sd[oc])
        home[...] = dot(shared, sd[c])
        home_copy.start()

    def sent_rails():
        home_x(c).wait_send()
        for d in range(2):

            @pl.when(has[d])
            def _():
                own_meta(d).wait_send()
                remote(xo.at[c], xl.at[z], own_ss.at[d], rail_rs.at[z, 0], ep, oc).wait_send()

        for lv in order:

            @pl.when(onward(lv)[0])
            def _():
                rail_meta(lv).wait_send()
                remote(xl.at[lv], xl.at[lv], rail_ss.at[lv], rail_rs.at[lv, 0], ep, oc).wait_send()

    def sent_deals(lv):
        met(lv).wait_send()
        dealt(lv).wait_send()

    def sent_back(lv, lone=False):
        if lone:
            one = ret.at[lv, 0]
            remote(one, one, ret_ss.at[lv], ret_rs.at[lv, 0], ep, oc).wait_send()
        else:
            all_handed(lv).wait_send()

    def sent_pair(whole):
        both = rh.at[pl.ds(0, 2)] if whole else rh.at[0]
        remote(both, both, rh_ss.at[0], rh_rs.at[0], ep, oc).wait_send()

    near0, near1, near2 = order
    def loaded():
        for load in loads:
            load.wait()

    @pl.when(at_end)
    def _():
        with jax.named_scope("gather0"):
            pick = meet(near0)
            for q in range(CHUNKS):
                step(near0, q, pick)
        loaded()
        pick = meet(near1)
        step(near1, 0, pick)
        with jax.named_scope("computez"):
            compute(z, "own")
        for s in range(BACKS):
            hand_own(s).start()
        step(near1, 1, pick)
        with jax.named_scope("compute0"):
            compute(near0, "pair")
        for s in range(BACKS):
            for h in range(2):
                hand_pair(near0, s, h, True).start()
        step(near1, 2, pick)
        step(near1, 3, pick)
        pick = meet(near2)
        step(near2, 0, pick)
        with jax.named_scope("compute1"):
            compute(near1, "far")
        send_back(near1, 0)
        step(near2, 1, pick)
        with jax.named_scope("share"):
            share()
        step(near2, 2, pick)
        with jax.named_scope("give1#s=0"):
            give(near1, 0)
        step(near2, 3, pick)
        send_back(near1, 1)
        with jax.named_scope("compute2"):
            compute(near2, "far")
        for s in range(BACKS):
            send_back(near2, s)
        send_back(near1, 2)
        send_back(near1, 3)
        with jax.named_scope("give1#s=1"):
            give(near1, 1)
        with jax.named_scope("sent"):
            sent_rails()
            for lv in (z, near0, near1):
                sent_deals(lv)
        for s in range(BACKS):
            with jax.named_scope(f"give2#s={s}"):
                give(near2, s)
            with jax.named_scope(f"cross#s={s}"):
                cross(s, False)
        for s in range(2, BACKS):
            with jax.named_scope(f"give1#s={s}"):
                give(near1, s)
        sent_pair(True)
        for lv in (near1, near2):
            sent_back(lv)
        sent_deals(near2)

    @pl.when(jnp.logical_not(at_end))
    def _():
        for lv in order:
            with jax.named_scope("gather"):
                pick = meet(lv)
                for q in range(CHUNKS):
                    step(lv, q, pick)
        loaded()
        with jax.named_scope("compute1"):
            compute(near1, "chain")
        for s in range(BACKS):
            for h in range(2):
                hand_pair(near1, s, h, False).start()
            hand(near1, 0, s).start()
        with jax.named_scope("compute0"):
            compute(near0, "far")
        for s in range(BACKS):
            send_back(near0, s)
        with jax.named_scope("computez"):
            compute(z, "own")
        for s in range(BACKS):
            hand_own(s).start()
        with jax.named_scope("share"):
            share()
        with jax.named_scope("compute2"):
            compute(near2, "far")
        for s in range(BACKS):
            send_back(near2, s)
        for s in range(BACKS):
            with jax.named_scope(f"cross#s={s}"):
                cross(s, True)
        for lv, s in (
            (near0, 0),
            (near0, 1),
            (near2, 0),
            (near2, 1),
            (near1, 0),
            (near2, 2),
            (near1, 1),
            (near2, 3),
            (near1, 2),
            (near0, 2),
            (near1, 3),
            (near0, 3),
        ):
            with jax.named_scope(f"give{0 if lv is near0 else 1 if lv is near1 else 2}#s={s}"):
                (give_chain if lv is near1 else give)(lv, s)
            if lv is near0 and s == 0:
                with jax.named_scope("sent"):
                    sent_rails()
                    for v in (z, *order):
                        sent_deals(v)
                    sent_back(near0)
        sent_pair(False)
        sent_back(near1, True)
        sent_back(near2)

    home_copy.wait_recv()
    home[...] += home_rx[...]
    square = [jnp.zeros((rows, 1), F32) for _ in range(2)]
    for s in range(BACKS):
        for k in range(2):

            @pl.when(at_end)
            def _():
                settle(s, k, False)

            @pl.when(jnp.logical_not(at_end))
            def _():
                settle(s, k, True)

            with jax.named_scope(f"wait_cross#s={s}"):
                cross_copy(s, k).wait_recv()
            acc[k] += cross_rx[s, k].astype(F32)
            for piece in pieces(s, k, rows):
                add(inner, s, k, piece)
            part = pl.ds(k * rows, rows)
            total = (home[part, ss(s)] + acc[k]).astype(BF16).astype(F32)
            home[part, ss(s)] = total
            square[k] += jnp.sum(total * total, axis=1, keepdims=True)
    for k in range(2):
        sq_send[k * rows : (k + 1) * rows, :] = jnp.broadcast_to(square[k], (rows, 128))
    squares = remote(sq_send, sq_rx, sq_ss.at[0], sq_rs.at[0], ep, oc)
    squares.start()
    with jax.named_scope("wait_sq"):
        squares.wait_recv()
    with jax.named_scope("final"):
      final = lax.rsqrt((sq_send[...] + sq_rx[...])[:, :1] / width + 1e-06)
      out_ref[...] = (home[...] * final * out_gain_ref[c]).astype(BF16)

    with jax.named_scope("sentend"):
        def passed(lv):
            some = rs_send.at[lv]
            remote(some, some, back_ss.at[lv], back_rs.at[lv, 0], ep, oc).wait_send()

        for lv in (near1, near2):
            passed(lv)

        @pl.when(jnp.logical_not(at_end))
        def _():
            passed(near0)

        remote(cross_tx, cross_tx, cross_ss.at[0], cross_rs.at[0, 0], ep, oc).wait_send()
        remote(ro.at[0], ro.at[0], ro_ss.at[0], ro_rs.at[0], ep, oc).wait_send()
        pair_met().wait_send()
        home_copy.wait_send()
        squares.wait_send()


def ladder_local(
    n,
    cap,
    tokens,
    expert_ids,
    gate_weights,
    norm_gain,
    expert_gate,
    expert_up,
    expert_down,
    shared_gate,
    shared_up,
    shared_down,
    out_gain,
):
    rows, width = tokens.shape
    topk = expert_ids.shape[1]
    ff = expert_gate.shape[2]
    sh = shared_gate.shape[1]
    cols = width // 2
    levels = n // 2
    rw = cols // BACKS
    dma = pltpu.SemaphoreType.DMA
    vmem = pl.BlockSpec(memory_space=pltpu.VMEM)
    hbm = pl.BlockSpec(memory_space=pl.ANY)
    return pl.pallas_call(
        functools.partial(ladder_kernel, n, cap),
        out_shape=pltpu.VMEM((2 * rows, cols), BF16),
        in_specs=[hbm] * 11,
        out_specs=vmem,
        scratch_shapes=[
            pltpu.VMEM((topk, rows), jnp.int32),
            pltpu.VMEM((topk, rows), F32),
            pltpu.VMEM((1, width), F32),
            pltpu.VMEM((2, 1, cols), F32),
            pltpu.VMEM((rows, width), BF16),
            pltpu.VMEM((2, rows, width), BF16),
            pltpu.VMEM((levels, rows, width), BF16),
            pltpu.VMEM((levels, levels, 8, rows), F32),
            pltpu.VMEM((levels, 4, 8, rows), F32),
            pltpu.VMEM((levels, 3, cap, width), BF16),
            pltpu.VMEM((levels, 4, cap, width), BF16),
            pltpu.VMEM((width, ff), BF16),
            pltpu.VMEM((width, ff), BF16),
            pltpu.VMEM((2, ff, cols), BF16),
            pltpu.VMEM((width, sh), BF16),
            pltpu.VMEM((width, sh), BF16),
            pltpu.VMEM((2, sh, cols), BF16),
            pltpu.VMEM((levels, 2, BACKS, 2, 2 * cap, rw), BF16),
            pltpu.VMEM((levels, 4, BACKS, 2 * cap, rw), BF16),
            pltpu.VMEM((levels, 2, rows, 4 * cap), BF16),
            pltpu.VMEM((2, rows, 2 * cap), BF16),
            pltpu.VMEM((2, 2, rows, 4 * cap), BF16),
            pltpu.VMEM((4, 8, rows), F32),
            pltpu.VMEM((2, BACKS, 2, 2 * cap, rw), BF16),
            pltpu.VMEM((2, BACKS, 2, 2 * cap, rw), BF16),
            pltpu.VMEM((BACKS, 2, rows, rw), BF16),
            pltpu.VMEM((BACKS, 2, rows, rw), BF16),
            pltpu.VMEM((2, rows, rw), F32),
            pltpu.VMEM((levels, BACKS, 2, rows, rw), BF16),
            pltpu.VMEM((levels + 1, BACKS, 2, rows, rw), BF16),
            pltpu.VMEM((2 * rows, cols), F32),
            pltpu.VMEM((2 * rows, cols), F32),
            pltpu.VMEM((2 * rows, cols), F32),
            pltpu.VMEM((2 * rows, 128), F32),
            pltpu.VMEM((2 * rows, 128), F32),
            dma((5,)),
            dma((8,)),
            dma((2,)),
            dma((levels,)),
            dma((levels, CHUNKS)),
            dma((2,)),
            dma((levels,)),
            dma((levels,)),
            dma((levels,)),
            dma((levels,)),
            dma((levels,)),
            dma((levels,)),
            dma((levels,)),
            dma((levels, BACKS)),
            dma((levels,)),
            dma((levels + 1, 2 * BACKS + 2)),
            dma((1,)),
            dma((1,)),
            dma((1,)),
            dma((BACKS,)),
            dma((1,)),
            dma((BACKS,)),
            dma((1,)),
            dma((BACKS, 2)),
            dma((1,)),
            dma((1,)),
            dma((1,)),
            dma((1,)),
            dma((1,)),
            dma((1,)),
        ],
        compiler_params=pltpu.CompilerParams(
            collective_id=0, has_side_effects=True, vmem_limit_bytes=60 * 1024 * 1024
        ),
    )(
        expert_ids.T,
        gate_weights.T,
        tokens,
        norm_gain.reshape(1, width),
        out_gain.reshape(2, 1, cols),
        expert_gate,
        expert_up,
        expert_down,
        shared_gate,
        shared_up,
        shared_down,
    )


TOPK = 4


def expert_work(received, expert_gate, expert_up, expert_down):
    gate = jnp.einsum("slcd,ldf->slcf", received, expert_gate, preferred_element_type=jnp.float32)
    upper = jnp.einsum("slcd,ldf->slcf", received, expert_up, preferred_element_type=jnp.float32)
    hidden = (jax.nn.silu(gate) * upper).astype(jnp.bfloat16)
    return jnp.einsum(
        "slcf,lfd->slcd", hidden, expert_down, preferred_element_type=jnp.float32
    ).astype(jnp.bfloat16)


def local(
    tokens,
    expert_ids,
    gate_weights,
    norm_gain,
    expert_gate,
    expert_up,
    expert_down,
    shared_gate,
    shared_up,
    shared_down,
    out_gain,
):
    local_rows = tokens.shape[0]
    width = tokens.shape[1]
    ep_count = lax.axis_size("ep")
    tp_count = lax.axis_size("tp")
    device_count = ep_count * tp_count
    local_experts = expert_gate.shape[0]
    expert_count = device_count * local_experts
    capacity = 3 * local_rows * TOPK // (2 * expert_count)
    values = tokens.astype(jnp.float32)
    scale = lax.rsqrt(jnp.mean(values * values, axis=1, keepdims=True) + 1e-06)
    normed = (values * scale * norm_gain).astype(jnp.bfloat16)
    flat_ids = expert_ids.reshape(-1)
    one_hot = (flat_ids[:, None] == jnp.arange(expert_count, dtype=jnp.int32)[None, :]).astype(
        jnp.int32
    )
    earlier = jnp.cumsum(one_hot, axis=0) - one_hot
    slot_index = jnp.sum(earlier * one_hot, axis=1)
    target = flat_ids * capacity + slot_index
    copy_rows = normed[jnp.arange(local_rows * TOPK, dtype=jnp.int32) // TOPK]
    outgoing = jnp.zeros((expert_count * capacity, width), jnp.bfloat16).at[target].set(copy_rows)
    sending = outgoing.reshape(device_count, local_experts * capacity, width)
    received = lax.all_to_all(sending, ("ep", "tp"), split_axis=0, concat_axis=0, tiled=True)
    received = received.reshape(device_count, local_experts, capacity, width)
    results = expert_work(received, expert_gate, expert_up, expert_down)
    results = results.reshape(device_count, local_experts * capacity, width)
    returned = lax.all_to_all(results, ("ep", "tp"), split_axis=0, concat_axis=0, tiled=True)
    returned = returned.reshape(expert_count * capacity, width)
    picked = returned[target].astype(jnp.float32).reshape(local_rows, TOPK, width)
    routed = jnp.sum(picked * gate_weights[:, :, None], axis=1)
    piece = lax.all_gather(normed, "tp", axis=0, tiled=True)
    gate = jnp.dot(piece, shared_gate, preferred_element_type=jnp.float32)
    upper = jnp.dot(piece, shared_up, preferred_element_type=jnp.float32)
    shared_hidden = (jax.nn.silu(gate) * upper).astype(jnp.bfloat16)
    shared_out = lax.psum_scatter(
        jnp.dot(shared_hidden, shared_down, preferred_element_type=jnp.float32),
        "tp",
        scatter_dimension=0,
        tiled=True,
    )
    mixed = (routed + shared_out).astype(jnp.bfloat16)
    mixed_values = mixed.astype(jnp.float32)
    final_scale = lax.rsqrt(jnp.mean(mixed_values * mixed_values, axis=1, keepdims=True) + 1e-06)
    normalized = (mixed_values * final_scale * out_gain).astype(jnp.bfloat16)
    return lax.all_to_all(normalized, "tp", split_axis=1, concat_axis=0, tiled=True)


def solution(mesh):
    in_specs = (
        P(("grp", "ep", "tp"), None),
        P(("grp", "ep", "tp"), None),
        P(("grp", "ep", "tp"), None),
        P(),
        P(("ep", "tp"), None, None),
        P(("ep", "tp"), None, None),
        P(("ep", "tp"), None, None),
        P(None, "tp"),
        P(None, "tp"),
        P("tp", None),
        P(),
    )
    out_specs = P(("grp", "ep"), "tp")
    n, tp = mesh.shape["ep"], mesh.shape["tp"]

    def run(*args):
        tokens, expert_gate = args[0], args[4]
        rows = tokens.shape[0] // mesh.size
        experts = expert_gate.shape[0]
        cap = 3 * rows * args[1].shape[1] // (2 * experts)
        dense = experts == n * tp and experts <= 8 * args[1].shape[1]
        dense = dense and tp == 2 and n == 8 and rows == 128 and cap % 16 == 0
        body = functools.partial(ladder_local, n, cap) if dense else local
        return jax.shard_map(
            body, mesh=mesh, in_specs=in_specs, out_specs=out_specs, check_vma=False
        )(*args)

    return run
```

```python
import functools

import jax
import jax.numpy as jnp
from jax import lax
from jax.experimental import pallas as pl
from jax.experimental.pallas import tpu as pltpu
from jax.sharding import PartitionSpec as P

MESH = pl.DeviceIdType.MESH
CHUNKS = 8
BACKS = 4


def pieces(s, k, rows):
    if s < BACKS - 1:
        return [(2 * s + k, 0, rows)]
    half = rows // 2
    return [(2 * s + 2 * k + i, i * half, half) for i in range(2)]
F32 = jnp.float32
BF16 = jnp.bfloat16


def ladder_kernel(
    n,
    cap,
    ids_hbm,
    gates_hbm,
    tok_hbm,
    gain_hbm,
    out_gain_hbm,
    eg_hbm,
    eu_hbm,
    ed_hbm,
    sg_hbm,
    su_hbm,
    sd_hbm,
    out_ref,
    ids_ref,
    gates_ref,
    gain_ref,
    out_gain_ref,
    tok,
    xo,
    xl,
    meta,
    mall,
    stage,
    xr,
    wg,
    wu,
    wd,
    sg,
    su,
    sd,
    res,
    ret,
    pt,
    pc,
    comb,
    mallp,
    rh,
    ro,
    cross_tx,
    cross_rx,
    acc,
    rs_send,
    rs_rx,
    home,
    home_send,
    home_rx,
    sq_send,
    sq_rx,
    tok_sem,
    load_sem,
    own_ss,
    rail_ss,
    rail_rs,
    mown_ss,
    mrail_ss,
    mrail_rs,
    md_ss,
    md_rs,
    disp_ss,
    disp_rs,
    ret_ss,
    ret_rs,
    back_ss,
    back_rs,
    mp_ss,
    mp_rs,
    rh_ss,
    rh_rs,
    ro_ss,
    ro_rs,
    cross_ss,
    cross_rs,
    ox_ss,
    ox_rs,
    h_ss,
    h_rs,
    sq_ss,
    sq_rs,
):
    levels = n // 2
    rows, width = tok.shape
    cols = width // 2
    cw, rw = width // CHUNKS, cols // BACKS
    topk = ids_ref.shape[0]
    per = 4
    experts = levels * per
    ep = lax.axis_index("ep")
    c = lax.axis_index("tp")
    oc = 1 - c
    x = ep % 2
    z = ep // 2
    ox = 1 - x
    across = z * 2 + ox
    mine = 2 * x + c
    others = (2 * x + oc, 2 * ox + c, 2 * ox + oc)
    homes = ((ep, oc), (across, c), (across, oc))
    has = (z < levels - 1, z > 0)
    beside = (jnp.minimum(ep + 2, n - 1), jnp.maximum(ep - 2, 0))
    at_end = (z == 0) | (z == levels - 1)

    firsts = [(ids_hbm, ids_ref), (gates_hbm, gates_ref), (tok_hbm, tok), (gain_hbm, gain_ref)]
    firsts.append((out_gain_hbm, out_gain_ref))
    firsts = [pltpu.make_async_copy(a, b, tok_sem.at[i]) for i, (a, b) in enumerate(firsts)]
    for load in firsts:
        load.start()

    def signal(e, core):
        pl.semaphore_signal(barrier, inc=1, device_id={"ep": e, "tp": core}, device_id_type=MESH)

    barrier = pltpu.get_barrier_semaphore()
    for e, core in homes:
        signal(e, core)
    for d in range(2):

        @pl.when(has[d])
        def _():
            signal(beside[d], c)

    loads = [
        (sg_hbm, sg),
        (su_hbm, su),
        (sd_hbm.at[:, pl.ds(0, cols)], sd.at[0]),
        (sd_hbm.at[:, pl.ds(cols, cols)], sd.at[1]),
        (eg_hbm.at[0], wg),
        (eu_hbm.at[0], wu),
        (ed_hbm.at[0, :, pl.ds(0, cols)], wd.at[0]),
        (ed_hbm.at[0, :, pl.ds(cols, cols)], wd.at[1]),
    ]
    loads = [pltpu.make_async_copy(s, d, load_sem.at[i]) for i, (s, d) in enumerate(loads)]
    def remote(src, dst, ssem, rsem, e, core):
        return pltpu.make_async_remote_copy(
            src_ref=src,
            dst_ref=dst,
            send_sem=ssem,
            recv_sem=rsem,
            device_id={"ep": e, "tp": core},
            device_id_type=MESH,
        )

    def dot(a, b):
        return jnp.dot(a, b, preferred_element_type=F32)

    def cs(q):
        return pl.ds(q * cw, cw)

    def ss(s):
        return pl.ds(s * rw, rw)

    for load in firsts[:2]:
        load.wait()
    expert = lax.broadcasted_iota(jnp.int32, (experts, rows), 0)
    dense = jnp.zeros((experts, rows), F32)
    member = jnp.zeros((experts, rows), F32)
    for k in range(topk):
        hit = ids_ref[k : k + 1, :] == expert
        dense += jnp.where(hit, gates_ref[k : k + 1, :], 0.0)
        member += jnp.where(hit, 1.0, 0.0)
    row = lax.broadcasted_iota(jnp.int32, (rows, rows), 0)
    lane = lax.broadcasted_iota(jnp.int32, (rows, rows), 1)
    earlier = jnp.where(row < lane, 1.0, 0.0).astype(BF16)
    eye = jnp.where(row == lane, 1.0, 0.0).astype(BF16)
    place = jnp.where(member > 0.0, dot(member.astype(BF16), earlier), -1.0)
    for k in range(levels):
        part = slice(k * per, (k + 1) * per)
        meta[z, k] = jnp.concatenate([dense[part], place[part]], axis=0)

    near = jnp.minimum(z, levels - 1 - z)
    sign = jnp.where(2 * z < levels - 1, 1, -1)
    order = []
    for i in range(levels - 1):
        paired = z + sign * (i // 2 + 1) * (1 - 2 * (i % 2))
        order.append(jnp.where(i < 2 * near, paired, z + sign * (i - near + 1)))

    pair = z + 1 - 2 * (z % 2)

    def own_rail(q, d):
        return remote(
            xo.at[c, :, cs(q)],
            xl.at[z, :, cs(q)],
            own_ss.at[d],
            rail_rs.at[z, q],
            beside[d],
            c,
        )

    def own_meta(d):
        return remote(meta.at[z], meta.at[z], mown_ss.at[d], mrail_rs.at[z], beside[d], c)

    def onward(lv):
        up = lv < z
        return jnp.where(up, has[0], has[1]), jnp.where(up, beside[0], beside[1])

    def rail(lv, q):
        return remote(
            xl.at[lv, :, cs(q)],
            xl.at[lv, :, cs(q)],
            rail_ss.at[lv],
            rail_rs.at[lv, q],
            onward(lv)[1],
            c,
        )

    def rail_meta(lv):
        return remote(
            meta.at[lv], meta.at[lv], mrail_ss.at[lv], mrail_rs.at[lv], onward(lv)[1], c
        )

    def deal_meta(lv, d):
        return remote(
            meta.at[lv, z], mall.at[lv, mine], md_ss.at[lv], md_rs.at[lv], *homes[d]
        )

    def met(lv):
        three = mall.at[lv, pl.ds(0, 3)]
        return remote(three, three, md_ss.at[lv], md_rs.at[lv], ep, oc)

    def deal(lv, d, q):
        return remote(
            stage.at[lv, d, :, cs(q)],
            xr.at[lv, mine, :, cs(q)],
            disp_ss.at[lv],
            disp_rs.at[lv],
            *homes[d],
        )

    def dealt(lv):
        return remote(
            stage.at[lv], xr.at[lv, pl.ds(0, 3)], disp_ss.at[lv], disp_rs.at[lv], ep, oc
        )

    def hand(lv, d, s):
        src = (
            res.at[lv, oc, s, x],
            res.at[lv, 0, s, ox],
            res.at[lv, 1, s, ox],
        )[d]
        e, core = ((ep, oc), (across, 0), (across, 1))[d]
        return remote(
            src, ret.at[lv, mine, s], ret_ss.at[lv], ret_rs.at[lv, s], e, core
        )

    def handed(lv, s):
        three = ret.at[lv, pl.ds(0, 3), s]
        return remote(three, three, ret_ss.at[lv], ret_rs.at[lv, s], ep, oc)

    def all_handed(lv):
        three = ret.at[lv, pl.ds(0, 3)]
        return remote(three, three, ret_ss.at[lv], ret_rs.at[lv, 0], ep, oc)

    def back(lv, s, k, piece):
        up = lv > z
        t = jnp.where(up, jnp.minimum(z + 1, levels - 1), jnp.maximum(z - 1, 0))
        i, first, count = piece
        return remote(
            rs_send.at[lv, s, k, pl.ds(first, count)],
            rs_rx.at[lv, s, k, pl.ds(first, count)],
            back_ss.at[lv],
            back_rs.at[lv, i],
            t * 2 + x,
            c,
        )

    def deal_pair(d):
        return remote(
            meta.at[z, pair], mallp.at[mine], mp_ss.at[0], mp_rs.at[0], *homes[d]
        )

    def pair_met():
        three = mallp.at[pl.ds(0, 3)]
        return remote(three, three, mp_ss.at[0], mp_rs.at[0], ep, oc)

    def hand_pair(lv, s, h, whole):
        src, dst = res.at[lv, h, s], rh.at[c, s]
        if not whole:
            src, dst = src.at[ox], dst.at[ox]
        return remote(src, dst, rh_ss.at[0], rh_rs.at[s], pair * 2 + x, h)

    def paired(s, whole):
        both = rh.at[pl.ds(0, 2), s] if whole else rh.at[pl.ds(0, 2), s, 0]
        return remote(both, both, rh_ss.at[0], rh_rs.at[s], ep, oc)

    def hand_own(s):
        return remote(res.at[z, oc, s], ro.at[c, s], ro_ss.at[0], ro_rs.at[s], ep, oc)

    def cross_copy(s, k):
        return remote(
            cross_tx.at[s, k],
            cross_rx.at[s, k],
            cross_ss.at[0],
            cross_rs.at[s, k],
            across,
            c,
        )

    def came(slot, s, k, piece):
        i, first, count = piece
        part = rs_rx.at[slot, s, k, pl.ds(first, count)]
        return remote(part, part, back_ss.at[0], back_rs.at[slot, i], ep, oc)

    home_x = lambda core: remote(xo.at[core], xo.at[core], ox_ss.at[0], ox_rs.at[0], ep, oc)

    def normalise(part):
        values = tok[part, :].astype(F32)
        scale = lax.rsqrt(jnp.mean(values * values, axis=1, keepdims=True) + 1e-06)
        xo[c, part, :] = (values * scale * gain_ref[...]).astype(BF16)

    with jax.named_scope("tokload"):
        for load in firsts[2:]:
            load.wait()
    with jax.named_scope("norm"):
        normalise(pl.ds(0, rows))
    pl.semaphore_wait(barrier, 3 + has[0].astype(jnp.int32) + has[1].astype(jnp.int32))
    for d in range(2):

        @pl.when(has[d])
        def _():
            own_meta(d).start()
            for q in range(CHUNKS):
                own_rail(q, d).start()

    slot_f = lax.broadcasted_iota(jnp.int32, (cap, rows), 0).astype(F32)

    def selection(lv):
        picks = [
            jnp.where(meta[lv, z, pl.ds(per + j, 1), :] == slot_f, 1.0, 0.0)
            for j in (mine, *others)
        ]
        return jnp.concatenate(picks, axis=0).astype(BF16)

    def spread_meta(lv):
        mall[lv, mine] = meta[lv, z]
        for d in range(3):
            deal_meta(lv, d).start()

    def spread(lv, q, pick, block):
        got = dot(pick, block).astype(BF16)
        xr[lv, mine, :, cs(q)] = got[:cap]
        for d in range(3):
            stage[lv, d, :, cs(q)] = got[(d + 1) * cap : (d + 2) * cap]
        for d in (1, 2, 0):
            deal(lv, d, q).start()

    spread_meta(z)
    mallp[mine] = meta[z, pair]
    for d in range(3):
        deal_pair(d).start()
    pick = selection(z)
    for q in range(CHUNKS):
        spread(z, q, pick, xo[c, :, cs(q)])
    home_x(c).start()
    for load in loads:
        load.start()

    def silu_mul(g, u):
        return (g / (1.0 + jnp.exp(-g)) * u).astype(BF16)

    def columns(m):
        return lax.dot_general(
            eye, m.astype(BF16), (((1,), (1,)), ((), ())), preferred_element_type=F32
        ).astype(jnp.int32)

    def two(m):
        col = columns(m)
        return [
            jnp.where(x == 0, col[:, per + j : per + j + 1], col[:, per + 2 + j : per + 3 + j])
            for j in range(2)
        ]

    def expander(wants):
        spot = lax.broadcasted_iota(jnp.int32, (rows, len(wants) * cap), 1)
        want = wants[0]
        for j in range(1, len(wants)):
            want = jnp.where(spot >= cap * j, wants[j] + cap * j, want)
        return jnp.where(want == spot, 1.0, 0.0).astype(BF16)

    def compute(lv, kind):
        met(lv).wait_recv()
        weight = jnp.concatenate(
            [
                jnp.sum(
                    jnp.where(
                        mall[lv, j, pl.ds(per + mine, 1), :] == slot_f,
                        mall[lv, j, pl.ds(mine, 1), :],
                        0.0,
                    ),
                    axis=1,
                    keepdims=True,
                )
                for j in range(per)
            ],
            axis=0,
        )
        for k in range(2):
            if kind == "far":
                col = columns(mall[lv, 2 * x + k])
                pt[lv, k] = expander([col[:, per + j : per + j + 1] for j in range(per)])
            elif kind == "chain":
                pc[k] = expander(two(mall[lv, 2 * x + k]))
        if kind == "own":
            pair_met().wait_recv()
            for r, rail_x in enumerate((x, ox)):
                for k in range(2):
                    j = 2 * rail_x + k
                    comb[r, k] = expander(two(mall[lv, j]) + two(mallp[j]))
        with jax.named_scope("wait_dealt"):
            dealt(lv).wait_recv()
        xs = xr[lv].reshape(per * cap, width)
        hidden = silu_mul(dot(xs, wg[...]), dot(xs, wu[...]))
        for s in range(BACKS):
            for h in range(2):
                out = (dot(hidden, wd[h, :, ss(s)]) * weight).astype(BF16)
                res[lv, h, s] = out.reshape(2, 2 * cap, rw)
            if kind in ("far", "chain"):
                ret[lv, mine, s] = res[lv, c, s, x]
            elif kind == "own":
                ro[c, s] = res[lv, c, s]

    def send_back(lv, s):
        for d in (1, 2, 0):
            hand(lv, d, s).start()

    def merge(lv, s, k):
        got = jnp.concatenate(
            [ret[lv, j, s, k * cap : (k + 1) * cap, :] for j in range(per)], axis=0
        )
        acc[k] = dot(pt[lv, k], got)

    def add(slot, s, k, piece):
        with jax.named_scope(f"wait_came#s={s}"):
            came(slot, s, k, piece).wait_recv()
        part = pl.ds(piece[1], piece[2])
        acc[k, part, :] += rs_rx[slot, s, k, part, :].astype(F32)

    def ready(lv, s):
        with jax.named_scope(f"wait_handed#s={s}"):
            handed(lv, s).wait_recv()

    def pass_on(lv, s, k, piece):
        part = pl.ds(piece[1], piece[2])
        rs_send[lv, s, k, part, :] = acc[k, part, :].astype(BF16)
        back(lv, s, k, piece).start()

    def give(lv, s):
        ready(lv, s)
        for k in range(2):
            merge(lv, s, k)
            for piece in pieces(s, k, rows):

                @pl.when(jnp.where(lv > z, has[1], has[0]))
                def _():
                    add(lv, s, k, piece)

                pass_on(lv, s, k, piece)

    def part_of(ref, j, s, r, k):
        return ref[j, s, r, k * cap : (k + 1) * cap, :]

    def give_chain(lv, s):
        one = ret.at[lv, 0, s]
        remote(one, one, ret_ss.at[lv], ret_rs.at[lv, s], ep, oc).wait_recv()
        for k in range(2):
            got = jnp.concatenate(
                [ret[lv, 2 * x + j, s, k * cap : (k + 1) * cap, :] for j in range(2)], axis=0
            )
            acc[k] = dot(pc[k], got)
            for piece in pieces(s, k, rows):
                add(lv, s, k, piece)
                pass_on(lv, s, k, piece)

    def cross(s, whole):
        hand = remote(ro.at[0, s], ro.at[0, s], ro_ss.at[0], ro_rs.at[s], ep, oc)
        hand.wait_recv()
        with jax.named_scope("wait_paired"):
            paired(s, whole).wait_recv()
        for k in range(2):
            got = jnp.concatenate(
                [part_of(ref, j, s, ox, k) for ref in (ro, rh) for j in range(2)], axis=0
            )
            cross_tx[s, k] = dot(comb[1, k], got).astype(BF16)
            cross_copy(s, k).start()

    def settle(s, k, whole):
        refs = (ro, rh) if whole else (ro,)
        got = jnp.concatenate([part_of(ref, j, s, x, k) for ref in refs for j in range(2)], axis=0)
        acc[k] = dot(comb[0, k, :, : got.shape[0]], got)

    def meet(lv):
        rail_meta(lv).wait_recv()

        @pl.when(onward(lv)[0])
        def _():
            rail_meta(lv).start()

        spread_meta(lv)
        return selection(lv)

    def steps(lv, i, pick):
        for q in range(i * CHUNKS // 4, (i + 1) * CHUNKS // 4):
            step(lv, q, pick)

    def step(lv, q, pick):
        with jax.named_scope(f"wait_rail#q={q}"):
            rail(lv, q).wait_recv()

        @pl.when(onward(lv)[0])
        def _():
            rail(lv, q).start()

        spread(lv, q, pick, xl[lv, :, cs(q)])

    home_copy = remote(home_send, home_rx, h_ss.at[0], h_rs.at[0], ep, oc)

    def share():
        home_x(oc).wait_recv()
        xs = xo[...].reshape(2 * rows, width)
        shared = silu_mul(dot(xs, sg[...]), dot(xs, su[...]))
        home_send[...] = dot(shared, sd[oc])
        home[...] = dot(shared, sd[c])
        home_copy.start()

    def sent_rails():
        home_x(c).wait_send()
        for d in range(2):

            @pl.when(has[d])
            def _():
                own_meta(d).wait_send()
                remote(xo.at[c], xl.at[z], own_ss.at[d], rail_rs.at[z, 0], ep, oc).wait_send()

        for lv in order:

            @pl.when(onward(lv)[0])
            def _():
                rail_meta(lv).wait_send()
                remote(xl.at[lv], xl.at[lv], rail_ss.at[lv], rail_rs.at[lv, 0], ep, oc).wait_send()

    def sent_deals(lv):
        met(lv).wait_send()
        dealt(lv).wait_send()

    def sent_back(lv, lone=False):
        if lone:
            one = ret.at[lv, 0]
            remote(one, one, ret_ss.at[lv], ret_rs.at[lv, 0], ep, oc).wait_send()
        else:
            all_handed(lv).wait_send()

    def sent_pair(whole):
        both = rh.at[pl.ds(0, 2)] if whole else rh.at[0]
        remote(both, both, rh_ss.at[0], rh_rs.at[0], ep, oc).wait_send()

    near0, near1, near2 = order
    def loaded():
        for load in loads:
            load.wait()

    @pl.when(at_end)
    def _():
        with jax.named_scope("gather0"):
            pick = meet(near0)
            for q in range(CHUNKS):
                step(near0, q, pick)
        loaded()
        pick = meet(near1)
        steps(near1, 0, pick)
        with jax.named_scope("computez"):
            compute(z, "own")
        for s in range(BACKS):
            hand_own(s).start()
        steps(near1, 1, pick)
        with jax.named_scope("compute0"):
            compute(near0, "pair")
        for s in range(BACKS):
            for h in range(2):
                hand_pair(near0, s, h, True).start()
        steps(near1, 2, pick)
        steps(near1, 3, pick)
        pick = meet(near2)
        steps(near2, 0, pick)
        with jax.named_scope("compute1"):
            compute(near1, "far")
        send_back(near1, 0)
        steps(near2, 1, pick)
        with jax.named_scope("share"):
            share()
        steps(near2, 2, pick)
        with jax.named_scope("give1#s=0"):
            give(near1, 0)
        steps(near2, 3, pick)
        send_back(near1, 1)
        with jax.named_scope("compute2"):
            compute(near2, "far")
        for s in range(BACKS):
            send_back(near2, s)
        send_back(near1, 2)
        send_back(near1, 3)
        with jax.named_scope("give1#s=1"):
            give(near1, 1)
        with jax.named_scope("sent"):
            sent_rails()
            for lv in (z, near0, near1):
                sent_deals(lv)
        for s in range(BACKS):
            with jax.named_scope(f"give2#s={s}"):
                give(near2, s)
            with jax.named_scope(f"cross#s={s}"):
                cross(s, False)
        for s in range(2, BACKS):
            with jax.named_scope(f"give1#s={s}"):
                give(near1, s)
        sent_pair(True)
        for lv in (near1, near2):
            sent_back(lv)
        sent_deals(near2)

    @pl.when(jnp.logical_not(at_end))
    def _():
        for lv in order:
            with jax.named_scope("gather"):
                pick = meet(lv)
                for q in range(CHUNKS):
                    step(lv, q, pick)
        loaded()
        with jax.named_scope("compute1"):
            compute(near1, "chain")
        for s in range(BACKS):
            for h in range(2):
                hand_pair(near1, s, h, False).start()
            hand(near1, 0, s).start()
        with jax.named_scope("compute0"):
            compute(near0, "far")
        for s in range(BACKS):
            send_back(near0, s)
        with jax.named_scope("computez"):
            compute(z, "own")
        for s in range(BACKS):
            hand_own(s).start()
        with jax.named_scope("share"):
            share()
        with jax.named_scope("compute2"):
            compute(near2, "far")
        for s in range(BACKS):
            send_back(near2, s)
        for s in range(BACKS):
            with jax.named_scope(f"cross#s={s}"):
                cross(s, True)
        for lv, s in (
            (near0, 0),
            (near0, 1),
            (near2, 0),
            (near2, 1),
            (near1, 0),
            (near2, 2),
            (near1, 1),
            (near2, 3),
            (near1, 2),
            (near0, 2),
            (near1, 3),
            (near0, 3),
        ):
            with jax.named_scope(f"give{0 if lv is near0 else 1 if lv is near1 else 2}#s={s}"):
                (give_chain if lv is near1 else give)(lv, s)
            if lv is near0 and s == 0:
                with jax.named_scope("sent"):
                    sent_rails()
                    for v in (z, *order):
                        sent_deals(v)
                    sent_back(near0)
        sent_pair(False)
        sent_back(near1, True)
        sent_back(near2)

    home_copy.wait_recv()
    home[...] += home_rx[...]
    square = [jnp.zeros((rows, 1), F32) for _ in range(2)]
    for s in range(BACKS):
        for k in range(2):

            @pl.when(at_end)
            def _():
                settle(s, k, False)

            @pl.when(jnp.logical_not(at_end))
            def _():
                settle(s, k, True)

            with jax.named_scope(f"wait_cross#s={s}"):
                cross_copy(s, k).wait_recv()
            acc[k] += cross_rx[s, k].astype(F32)
            for piece in pieces(s, k, rows):
                add(z, s, k, piece)
            part = pl.ds(k * rows, rows)
            total = (home[part, ss(s)] + acc[k]).astype(BF16).astype(F32)
            home[part, ss(s)] = total
            square[k] += jnp.sum(total * total, axis=1, keepdims=True)
    for k in range(2):
        sq_send[k * rows : (k + 1) * rows, :] = jnp.broadcast_to(square[k], (rows, 128))
    squares = remote(sq_send, sq_rx, sq_ss.at[0], sq_rs.at[0], ep, oc)
    squares.start()
    with jax.named_scope("wait_sq"):
        squares.wait_recv()
    with jax.named_scope("final"):
      final = lax.rsqrt((sq_send[...] + sq_rx[...])[:, :1] / width + 1e-06)
      out_ref[...] = (home[...] * final * out_gain_ref[c]).astype(BF16)

    with jax.named_scope("sentend"):
        def passed(lv):
            some = rs_send.at[lv]
            remote(some, some, back_ss.at[lv], back_rs.at[lv, 0], ep, oc).wait_send()

        for lv in (near1, near2):
            passed(lv)

        @pl.when(jnp.logical_not(at_end))
        def _():
            passed(near0)

        remote(cross_tx, cross_tx, cross_ss.at[0], cross_rs.at[0, 0], ep, oc).wait_send()
        remote(ro.at[0], ro.at[0], ro_ss.at[0], ro_rs.at[0], ep, oc).wait_send()
        pair_met().wait_send()
        home_copy.wait_send()
        squares.wait_send()


def ladder_local(
    n,
    cap,
    tokens,
    expert_ids,
    gate_weights,
    norm_gain,
    expert_gate,
    expert_up,
    expert_down,
    shared_gate,
    shared_up,
    shared_down,
    out_gain,
):
    rows, width = tokens.shape
    topk = expert_ids.shape[1]
    ff = expert_gate.shape[2]
    sh = shared_gate.shape[1]
    cols = width // 2
    levels = n // 2
    rw = cols // BACKS
    dma = pltpu.SemaphoreType.DMA
    vmem = pl.BlockSpec(memory_space=pltpu.VMEM)
    hbm = pl.BlockSpec(memory_space=pl.ANY)
    return pl.pallas_call(
        functools.partial(ladder_kernel, n, cap),
        out_shape=pltpu.VMEM((2 * rows, cols), BF16),
        in_specs=[hbm] * 11,
        out_specs=vmem,
        scratch_shapes=[
            pltpu.VMEM((topk, rows), jnp.int32),
            pltpu.VMEM((topk, rows), F32),
            pltpu.VMEM((1, width), F32),
            pltpu.VMEM((2, 1, cols), F32),
            pltpu.VMEM((rows, width), BF16),
            pltpu.VMEM((2, rows, width), BF16),
            pltpu.VMEM((levels, rows, width), BF16),
            pltpu.VMEM((levels, levels, 8, rows), F32),
            pltpu.VMEM((levels, 4, 8, rows), F32),
            pltpu.VMEM((levels, 3, cap, width), BF16),
            pltpu.VMEM((levels, 4, cap, width), BF16),
            pltpu.VMEM((width, ff), BF16),
            pltpu.VMEM((width, ff), BF16),
            pltpu.VMEM((2, ff, cols), BF16),
            pltpu.VMEM((width, sh), BF16),
            pltpu.VMEM((width, sh), BF16),
            pltpu.VMEM((2, sh, cols), BF16),
            pltpu.VMEM((levels, 2, BACKS, 2, 2 * cap, rw), BF16),
            pltpu.VMEM((levels, 4, BACKS, 2 * cap, rw), BF16),
            pltpu.VMEM((levels, 2, rows, 4 * cap), BF16),
            pltpu.VMEM((2, rows, 2 * cap), BF16),
            pltpu.VMEM((2, 2, rows, 4 * cap), BF16),
            pltpu.VMEM((4, 8, rows), F32),
            pltpu.VMEM((2, BACKS, 2, 2 * cap, rw), BF16),
            pltpu.VMEM((2, BACKS, 2, 2 * cap, rw), BF16),
            pltpu.VMEM((BACKS, 2, rows, rw), BF16),
            pltpu.VMEM((BACKS, 2, rows, rw), BF16),
            pltpu.VMEM((2, rows, rw), F32),
            pltpu.VMEM((levels, BACKS, 2, rows, rw), BF16),
            pltpu.VMEM((levels, BACKS, 2, rows, rw), BF16),
            pltpu.VMEM((2 * rows, cols), F32),
            pltpu.VMEM((2 * rows, cols), F32),
            pltpu.VMEM((2 * rows, cols), F32),
            pltpu.VMEM((2 * rows, 128), F32),
            pltpu.VMEM((2 * rows, 128), F32),
            dma((5,)),
            dma((8,)),
            dma((2,)),
            dma((levels,)),
            dma((levels, CHUNKS)),
            dma((2,)),
            dma((levels,)),
            dma((levels,)),
            dma((levels,)),
            dma((levels,)),
            dma((levels,)),
            dma((levels,)),
            dma((levels,)),
            dma((levels, BACKS)),
            dma((levels,)),
            dma((levels, 2 * BACKS + 2)),
            dma((1,)),
            dma((1,)),
            dma((1,)),
            dma((BACKS,)),
            dma((1,)),
            dma((BACKS,)),
            dma((1,)),
            dma((BACKS, 2)),
            dma((1,)),
            dma((1,)),
            dma((1,)),
            dma((1,)),
            dma((1,)),
            dma((1,)),
        ],
        compiler_params=pltpu.CompilerParams(
            collective_id=0, has_side_effects=True, vmem_limit_bytes=60 * 1024 * 1024
        ),
    )(
        expert_ids.T,
        gate_weights.T,
        tokens,
        norm_gain.reshape(1, width),
        out_gain.reshape(2, 1, cols),
        expert_gate,
        expert_up,
        expert_down,
        shared_gate,
        shared_up,
        shared_down,
    )


TOPK = 4


def expert_work(received, expert_gate, expert_up, expert_down):
    gate = jnp.einsum("slcd,ldf->slcf", received, expert_gate, preferred_element_type=jnp.float32)
    upper = jnp.einsum("slcd,ldf->slcf", received, expert_up, preferred_element_type=jnp.float32)
    hidden = (jax.nn.silu(gate) * upper).astype(jnp.bfloat16)
    return jnp.einsum(
        "slcf,lfd->slcd", hidden, expert_down, preferred_element_type=jnp.float32
    ).astype(jnp.bfloat16)


def local(
    tokens,
    expert_ids,
    gate_weights,
    norm_gain,
    expert_gate,
    expert_up,
    expert_down,
    shared_gate,
    shared_up,
    shared_down,
    out_gain,
):
    local_rows = tokens.shape[0]
    width = tokens.shape[1]
    ep_count = lax.axis_size("ep")
    tp_count = lax.axis_size("tp")
    device_count = ep_count * tp_count
    local_experts = expert_gate.shape[0]
    expert_count = device_count * local_experts
    capacity = 3 * local_rows * TOPK // (2 * expert_count)
    values = tokens.astype(jnp.float32)
    scale = lax.rsqrt(jnp.mean(values * values, axis=1, keepdims=True) + 1e-06)
    normed = (values * scale * norm_gain).astype(jnp.bfloat16)
    flat_ids = expert_ids.reshape(-1)
    one_hot = (flat_ids[:, None] == jnp.arange(expert_count, dtype=jnp.int32)[None, :]).astype(
        jnp.int32
    )
    earlier = jnp.cumsum(one_hot, axis=0) - one_hot
    slot_index = jnp.sum(earlier * one_hot, axis=1)
    target = flat_ids * capacity + slot_index
    copy_rows = normed[jnp.arange(local_rows * TOPK, dtype=jnp.int32) // TOPK]
    outgoing = jnp.zeros((expert_count * capacity, width), jnp.bfloat16).at[target].set(copy_rows)
    sending = outgoing.reshape(device_count, local_experts * capacity, width)
    received = lax.all_to_all(sending, ("ep", "tp"), split_axis=0, concat_axis=0, tiled=True)
    received = received.reshape(device_count, local_experts, capacity, width)
    results = expert_work(received, expert_gate, expert_up, expert_down)
    results = results.reshape(device_count, local_experts * capacity, width)
    returned = lax.all_to_all(results, ("ep", "tp"), split_axis=0, concat_axis=0, tiled=True)
    returned = returned.reshape(expert_count * capacity, width)
    picked = returned[target].astype(jnp.float32).reshape(local_rows, TOPK, width)
    routed = jnp.sum(picked * gate_weights[:, :, None], axis=1)
    piece = lax.all_gather(normed, "tp", axis=0, tiled=True)
    gate = jnp.dot(piece, shared_gate, preferred_element_type=jnp.float32)
    upper = jnp.dot(piece, shared_up, preferred_element_type=jnp.float32)
    shared_hidden = (jax.nn.silu(gate) * upper).astype(jnp.bfloat16)
    shared_out = lax.psum_scatter(
        jnp.dot(shared_hidden, shared_down, preferred_element_type=jnp.float32),
        "tp",
        scatter_dimension=0,
        tiled=True,
    )
    mixed = (routed + shared_out).astype(jnp.bfloat16)
    mixed_values = mixed.astype(jnp.float32)
    final_scale = lax.rsqrt(jnp.mean(mixed_values * mixed_values, axis=1, keepdims=True) + 1e-06)
    normalized = (mixed_values * final_scale * out_gain).astype(jnp.bfloat16)
    return lax.all_to_all(normalized, "tp", split_axis=1, concat_axis=0, tiled=True)


def solution(mesh):
    in_specs = (
        P(("grp", "ep", "tp"), None),
        P(("grp", "ep", "tp"), None),
        P(("grp", "ep", "tp"), None),
        P(),
        P(("ep", "tp"), None, None),
        P(("ep", "tp"), None, None),
        P(("ep", "tp"), None, None),
        P(None, "tp"),
        P(None, "tp"),
        P("tp", None),
        P(),
    )
    out_specs = P(("grp", "ep"), "tp")
    n, tp = mesh.shape["ep"], mesh.shape["tp"]

    def run(*args):
        tokens, expert_gate = args[0], args[4]
        rows = tokens.shape[0] // mesh.size
        experts = expert_gate.shape[0]
        cap = 3 * rows * args[1].shape[1] // (2 * experts)
        dense = experts == n * tp and experts <= 8 * args[1].shape[1]
        dense = dense and tp == 2 and n == 8 and rows == 128 and cap % 16 == 0
        body = functools.partial(ladder_local, n, cap) if dense else local
        return jax.shard_map(
            body, mesh=mesh, in_specs=in_specs, out_specs=out_specs, check_vma=False
        )(*args)

    return run
```
